32 devices in a mesh: fs: 8 (over z, x), tp: 4 (over y, core).
Axes of the slice: x: 2, y: 2, z: 4, core: 2. Of those that a mesh axis runs over, the one named last changes fastest.
Arguments:
- later_input: bfloat16 [4096, 2048], P(('fs', 'tp')), may hold values from -6 to 6
- saved_input: bfloat16 [4096, 2048], P(('fs', 'tp')), may hold values from -6 to 6
- cotangent: bfloat16 [4096, 3072], P('fs', 'tp'), may hold values from -6 to 6
- up_weight: bfloat16 [2048, 3072], P('fs', 'tp'), may hold values from -0.125 to 0.125
- gate_weight: bfloat16 [2048, 3072], P('fs', 'tp'), may hold values from -0.125 to 0.125
- up_taps: bfloat16 [3, 3072], replicated, may hold values from -3.5 to 3.5
- gate_taps: bfloat16 [3, 3072], replicated, may hold values from -3.5 to 3.5
- up_grad_sum: float32 [2048, 3072], P('fs', 'tp'), may hold values from -6 to 6
- gate_grad_sum: float32 [2048, 3072], P('fs', 'tp'), may hold values from -6 to 6
- up_taps_sum: float32 [3, 3072], replicated, may hold values from -6 to 6
- gate_taps_sum: float32 [3, 3072], replicated, may hold values from -6 to 6
Outputs:
- hidden: bfloat16 [4096, 3072], P('fs', 'tp')
- input_grad: bfloat16 [4096, 2048], P(('fs', 'tp'))
- new_up_sum: float32 [2048, 3072], P('fs', 'tp')
- new_gate_sum: float32 [2048, 3072], P('fs', 'tp')
- new_up_taps_sum: float32 [3, 3072], replicated
- new_gate_taps_sum: float32 [3, 3072], replicated
The draws below stay inside these ranges and needn't reach their ends.
All inputs are finite; a program needn't handle non-finite values.
Results may differ from the reference program's by a relative error of at most 0.018.
Values may be sent and summed in bfloat16 or wider, within the bound.
A program may use at most 64 MiB of HBM per device.

```python
import jax
import jax.numpy as jnp
from jax import lax

D = 2048
FF = 3072
TOKENS = 4096
N_FS = 8
N_TP = 4


def raised(array, key, source, target, blocks, factor):
    def block_of(axis_at):
        return (jnp.arange(array.shape[axis_at]) // (array.shape[axis_at] // blocks)).reshape((-1,) + (1,) * (array.ndim - 1 - axis_at))

    near = jax.random.permutation(key, blocks)[block_of(target)]
    other_side = (block_of(target) + blocks // 2) % blocks
    return jnp.where((block_of(source) == near) | (block_of(source) == other_side), factor * array, array)


def level_of(own_key, extent, shards, least, largest):
    loudness = 1.0
    for dim, shards_of in shards:
        steps = jax.random.uniform(jax.random.fold_in(jax.random.fold_in(own_key, 6), dim), (shards_of,), jnp.float32, least / len(shards), largest / len(shards))
        loudness = loudness * jnp.repeat(jnp.exp(steps), extent[dim] // shards_of).reshape((-1,) + (1,) * (len(extent) - 1 - dim))
    return loudness


def noise(rng, shape, deviation, limit, shards=(), dtype=jnp.bfloat16):
    result = deviation * jax.random.normal(rng, shape, jnp.float32)
    if shards:
        result = result * level_of(rng, shape, shards, -0.22, 0.18)
    return jnp.clip(result, -limit, limit).astype(dtype)


def noise_with(rng, extent, spread, reach, pieces, heavy, dtype=jnp.bfloat16):
    drawn = spread * jax.random.normal(rng, extent, jnp.float32)
    if pieces:
        drawn = drawn * level_of(rng, extent, pieces, -0.22, 0.18)
    return jnp.clip(raised(drawn, jax.random.fold_in(rng, 3), *heavy), -reach, reach).astype(dtype)


def setup_inputs(seed: int = 0) -> dict:
    splits = jax.random.split(jax.random.key(seed), 12)
    return {
        "later_input": noise(splits[0], (TOKENS, D), 1.0, 6.0, ((0, 32),)),
        "saved_input": noise_with(splits[1], (TOKENS, D), 1.0, 6.0, ((0, 32),), (0, 1, 32, 2.75)),
        "cotangent": noise_with(splits[2], (TOKENS, FF), 1.0, 6.0, ((0, 8), (1, 4)), (1, 0, 8, 2.0)),
        "up_weight": noise(splits[3], (D, FF), D ** -0.5, 0.125, ((0, 8), (1, 4))),
        "gate_weight": noise(splits[4], (D, FF), D ** -0.5, 0.125, ((0, 8), (1, 4))),
        "up_taps": noise(splits[5], (3, FF), 3 ** -0.5, 3.5),
        "gate_taps": noise(splits[6], (3, FF), 3 ** -0.5, 3.5),
        "up_grad_sum": noise(splits[7], (D, FF), 1.0, 6.0, ((0, 8), (1, 4)), jnp.float32),
        "gate_grad_sum": noise(splits[8], (D, FF), 1.0, 6.0, ((0, 8), (1, 4)), jnp.float32),
        "up_taps_sum": noise(splits[9], (3, FF), 1.0, 6.0, (), jnp.float32),
        "gate_taps_sum": noise(splits[10], (3, FF), 1.0, 6.0, (), jnp.float32),
    }


def delayed(values, steps):
    zeros = jnp.zeros_like(values[:steps])
    return jnp.concatenate([zeros, values[:-steps]], axis=0)

def advanced(values, steps):
    zeros = jnp.zeros_like(values[:steps])
    return jnp.concatenate([values[steps:], zeros], axis=0)

def depthwise(values, taps):
    return taps[2] * values + taps[1] * delayed(values, 1) + taps[0] * delayed(values, 2)

def depthwise_back(grads, taps):
    return taps[2] * grads + taps[1] * advanced(grads, 1) + taps[0] * advanced(grads, 2)

def taps_grad(grads, values):
    return jnp.stack([lax.optimization_barrier(jnp.sum(grads * delayed(values, 2), axis=0)), lax.optimization_barrier(jnp.sum(grads * delayed(values, 1), axis=0)), lax.optimization_barrier(jnp.sum(grads * values, axis=0))], axis=0)

def reference(later_input, saved_input, cotangent, up_weight, gate_weight, up_taps, gate_taps, up_grad_sum, gate_grad_sum, up_taps_sum, gate_taps_sum):
    tokens_all = later_input.shape[0]
    model_width = later_input.shape[1]
    hidden_units = up_weight.shape[1]
    seq_len = tokens_all // N_FS
    block_cols = hidden_units // N_TP
    grad_scale = jnp.float32(tokens_all ** (-0.5))
    taps_up = up_taps.astype(jnp.float32)
    taps_gate = gate_taps.astype(jnp.float32)

    def group(carry, inputs):
        sum_up, sum_gate, sum_taps_up, sum_taps_gate = carry
        later_rows, saved_rows, upstream = inputs
        up_later = jnp.dot(later_rows, up_weight, preferred_element_type=jnp.float32).astype(jnp.bfloat16)
        gate_later = jnp.dot(later_rows, gate_weight, preferred_element_type=jnp.float32).astype(jnp.bfloat16)
        conv_up = depthwise(up_later.astype(jnp.float32), taps_up)
        conv_gate = depthwise(gate_later.astype(jnp.float32), taps_gate)
        hidden_rows = (jax.nn.silu(conv_gate) * conv_up).astype(jnp.bfloat16)
        up_saved = jnp.dot(saved_rows, up_weight, preferred_element_type=jnp.float32).astype(jnp.bfloat16)
        gate_saved = jnp.dot(saved_rows, gate_weight, preferred_element_type=jnp.float32).astype(jnp.bfloat16)
        up_saved32 = up_saved.astype(jnp.float32)
        gate_saved32 = gate_saved.astype(jnp.float32)
        saved_up = depthwise(up_saved32, taps_up)
        saved_gate = depthwise(gate_saved32, taps_gate)
        sigmoid_gate = jax.nn.sigmoid(saved_gate)
        upstream32 = upstream.astype(jnp.float32)
        grad_conv_up = upstream32 * jax.nn.silu(saved_gate)
        grad_conv_gate = upstream32 * saved_up * sigmoid_gate * (1.0 + saved_gate * (1.0 - sigmoid_gate))
        grad_up = depthwise_back(grad_conv_up, taps_up).astype(jnp.bfloat16)
        grad_gate = depthwise_back(grad_conv_gate, taps_gate).astype(jnp.bfloat16)
        total = jnp.zeros((seq_len, model_width), jnp.float32)
        for block in range(N_TP):
            lower = block * block_cols
            upper = lower + block_cols
            partial_sum = jnp.dot(grad_up[:, lower:upper], up_weight[:, lower:upper].T, preferred_element_type=jnp.float32)
            partial_sum = partial_sum + jnp.dot(grad_gate[:, lower:upper], gate_weight[:, lower:upper].T, preferred_element_type=jnp.float32)
            rounded = lax.optimization_barrier(partial_sum.astype(jnp.bfloat16))
            total = total + rounded.astype(jnp.float32)
        dims = (((0,), (0,)), ((), ()))
        sum_up = sum_up + lax.dot_general(saved_rows, grad_up, dims, preferred_element_type=jnp.float32)
        sum_gate = sum_gate + lax.dot_general(saved_rows, grad_gate, dims, preferred_element_type=jnp.float32)
        sum_taps_up = sum_taps_up + taps_grad(grad_conv_up, up_saved32)
        sum_taps_gate = sum_taps_gate + taps_grad(grad_conv_gate, gate_saved32)
        return ((sum_up, sum_gate, sum_taps_up, sum_taps_gate), (hidden_rows, total.astype(jnp.bfloat16)))
    init = (jnp.zeros(up_weight.shape, jnp.float32), jnp.zeros(gate_weight.shape, jnp.float32), jnp.zeros(up_taps.shape, jnp.float32), jnp.zeros(gate_taps.shape, jnp.float32))
    inputs = (later_input.reshape(N_FS, seq_len, model_width), saved_input.reshape(N_FS, seq_len, model_width), cotangent.reshape(N_FS, seq_len, hidden_units))
    sums, outputs = lax.scan(group, init, inputs)
    hidden = outputs[0].reshape(tokens_all, hidden_units)
    input_grad = outputs[1].reshape(tokens_all, model_width)
    new_up_sum = up_grad_sum + grad_scale * sums[0]
    new_gate_sum = gate_grad_sum + grad_scale * sums[1]
    new_up_taps_sum = up_taps_sum + grad_scale * sums[2]
    new_gate_taps_sum = gate_taps_sum + grad_scale * sums[3]
    return (hidden, input_grad, new_up_sum, new_gate_sum, new_up_taps_sum, new_gate_taps_sum)
```

```python
import functools

import jax
import jax.numpy as jnp
from jax import lax
from jax.experimental import pallas as pl
from jax.experimental.pallas import tpu as pltpu
from jax.sharding import PartitionSpec as P

MESH = pl.DeviceIdType.MESH
F32 = jnp.float32
BF16 = jnp.bfloat16
CORES = 2


def tile_of(extent):
    return 256 if extent % 256 == 0 else 128


def pick(index, table):
    value = jnp.int32(table[0])
    for at in range(1, len(table)):
        value = jnp.where(index == at, jnp.int32(table[at]), value)
    return value


def near_order(z, nz):
    order = [z]
    for step in range(1, nz):
        order += [b for b in (z - step, z + step) if 0 <= b < nz]
    return order


def far_order(z, nz):
    need = {b: (nz - 1 - b) + z if b > z else b + (nz - 1 - z) for b in range(nz) if b != z}
    return sorted(need, key=lambda b: (need[b], -abs(b - z))) + [z]


def delayed(values, steps, row):
    return jnp.where(row >= steps, pltpu.roll(values, steps, 0), 0.0)


def advanced(values, steps, row):
    extent = values.shape[0]
    return jnp.where(row < extent - steps, pltpu.roll(values, extent - steps, 0), 0.0)


def kernel(
    nx, nz, nt,
    later_hbm, saved_hbm, cot_hbm, upw_hbm, gatew_hbm, taps_ref,
    hidden_ref, ingrad_ref, wsum_ref, tapsum_ref,
    weights, rows_l, rows_s, cot, acc_l, acc_s, gproj, gbuf, xrecv, uprecv, dnrecv,
    pbuf, precv, tloc, trecv,
    local_sem, w_recv, w_up, w_dn, w_x, r_recv, r_send, r_fwd,
    x_send, x_recv, up_send, up_recv, dn_send, dn_recv, p_send, p_recv,
    t_send, t_recv, tt_send, tt_recv,
):
    nf = nx * nz
    me = lax.axis_index("fs")
    tp = lax.axis_index("tp")
    x = lax.rem(me, nx)
    z = lax.div(me, nx)
    core = lax.rem(tp, CORES)
    chip = lax.div(tp, CORES)
    chips = nt // CORES
    depth = weights.shape[0] // nf
    both = weights.shape[1]
    cols = both // 2
    seq, width = rows_s.shape
    part = seq // nt

    def remote(src, dst, send, recv, f, t):
        return pltpu.make_async_remote_copy(
            src_ref=src, dst_ref=dst, send_sem=send, recv_sem=recv,
            device_id={"fs": f, "tp": t}, device_id_type=MESH,
        )

    def wblock(b):
        return weights.at[pl.ds(pl.multiple_of(b * depth, depth), depth), :]

    def rblock(ref, t):
        return ref.at[pl.ds(pl.multiple_of(t * part, part), part), :]

    own_w = [
        pltpu.make_async_copy(upw_hbm, wblock(me).at[:, pl.ds(0, cols)], local_sem.at[0]),
        pltpu.make_async_copy(gatew_hbm, wblock(me).at[:, pl.ds(cols, cols)], local_sem.at[1]),
    ]
    own_r = [
        pltpu.make_async_copy(saved_hbm, rblock(rows_s, tp), local_sem.at[2]),
        pltpu.make_async_copy(later_hbm, rblock(rows_l, tp), local_sem.at[3]),
    ]
    own_c = pltpu.make_async_copy(cot_hbm, cot, local_sem.at[4])
    for copy in own_w + own_r + [own_c]:
        copy.start()

    barrier = pltpu.get_barrier_semaphore()
    for d in range(1, nf):
        pl.semaphore_signal(
            barrier, inc=1, device_id={"fs": lax.rem(me + d, nf), "tp": tp}, device_id_type=MESH
        )
    for d in range(1, nt):
        pl.semaphore_signal(
            barrier, inc=1, device_id={"fs": me, "tp": lax.rem(tp + d, nt)}, device_id_type=MESH
        )
    pl.semaphore_wait(barrier, nf - 1 + nt - 1)

    def up_copy(b):
        return remote(wblock(b * nx + x), wblock(b * nx + x), w_up.at[b], w_recv.at[b * nx + x], me + nx, tp)

    def dn_copy(b):
        return remote(wblock(b * nx + x), wblock(b * nx + x), w_dn.at[b], w_recv.at[b * nx + x], me - nx, tp)

    def x_copies(b):
        return [
            remote(
                wblock(b * nx + x), wblock(b * nx + x), w_x.at[d - 1, b],
                w_recv.at[b * nx + x], z * nx + lax.rem(x + d, nx), tp,
            )
            for d in range(1, nx)
        ]

    def w_arrived(b):
        remote(wblock(b), wblock(b), w_up.at[0], w_recv.at[b], me, tp).wait_recv()

    for copy in own_w:
        copy.wait()

    @pl.when(z < nz - 1)
    def _():
        up_copy(z).start()

    @pl.when(z > 0)
    def _():
        dn_copy(z).start()

    for copy in x_copies(z):
        copy.start()

    for copy in own_r:
        copy.wait()
    rows = [rows_s, rows_l]
    mate = chip * CORES + (CORES - 1 - core)

    def row_copy(a, owner, target, sem):
        return remote(rblock(rows[a], owner), rblock(rows[a], owner), sem, r_recv.at[a, owner], me, target)

    def row_arrived(a, owner):
        row_copy(a, owner, tp, r_send.at[0, 0]).wait_recv()

    first_rows = []
    for a in range(2):
        for d in range(1, chips):
            target = lax.rem(chip + d, chips) * CORES + core
            first_rows.append(row_copy(a, tp, target, r_send.at[a, d]))
        first_rows.append(row_copy(a, tp, mate, r_send.at[a, 0]))
    for copy in first_rows:
        copy.start()

    whole = depth % 128 != 0

    def project(b, first=False, size=1):
        rows_of = size * depth
        at = pl.ds(pl.multiple_of(b * depth, rows_of), rows_of)
        step = tile_of(both)

        def body(j, carry):
            tile = pl.ds(pl.multiple_of(j * step, step), step)
            w = weights[at, tile]
            for r, acc in ((rows_s, acc_s), (rows_l, acc_l)):
                term = jnp.dot(r[:, at], w, preferred_element_type=F32)
                if first:
                    acc[:, tile] = term
                else:
                    acc[:, tile] += term
            return carry

        lax.fori_loop(0, both // step, body, 0)

    nears = [near_order(at, nz) for at in range(nz)]
    forwards = []
    for step in range(nz + 1):
        if 0 < step < nz:
            low, high = z - step, z + step

            @pl.when(low >= 0)
            def _():
                w_arrived(low * nx + x)

                @pl.when(z < nz - 1)
                def _():
                    up_copy(low).start()

                for copy in x_copies(low):
                    copy.start()

            @pl.when(high < nz)
            def _():
                w_arrived(high * nx + x)

                @pl.when(z > 0)
                def _():
                    dn_copy(high).start()

                for copy in x_copies(high):
                    copy.start()

        if step == 1:
            for a in range(2):
                for d in range(1, chips):
                    owner = lax.rem(chip + d, chips) * CORES + core
                    row_arrived(a, owner)
                    copy = row_copy(a, owner, mate, r_fwd.at[a, d])
                    copy.start()
                    forwards.append(copy)
            for a in range(2):
                for d in range(chips):
                    row_arrived(a, lax.rem(chip + d, chips) * CORES + (CORES - 1 - core))
            if not whole:
                project(me, first=True)
        if 0 < step < nz and not whole:

            @pl.when(low >= 0)
            def _():
                project(low * nx + x)

            @pl.when(high < nz)
            def _():
                project(high * nx + x)

        if step > 0:
            b = pick(z, [order[step - 1] for order in nears])
            for d in range(1, nx):
                block = b * nx + lax.rem(x + d, nx)
                w_arrived(block)
                if not whole:
                    project(block)
            if whole:
                project(b * nx, first=step == 1, size=nx)

    own_c.wait()
    lanes = 128

    def taps_of(at):
        return [taps_ref[k : k + 1, at] for k in range(3)]

    def conv(values, taps, row):
        return taps[2] * values + taps[1] * delayed(values, 1, row) + taps[0] * delayed(values, 2, row)

    def conv_back(grads, taps, row):
        return taps[2] * grads + taps[1] * advanced(grads, 1, row) + taps[0] * advanced(grads, 2, row)

    tloc[...] = jnp.zeros_like(tloc)

    def backward(j, carry):
        row = lax.broadcasted_iota(jnp.int32, (seq, lanes), 0)
        at_u = pl.ds(pl.multiple_of(j * lanes, lanes), lanes)
        at_g = pl.ds(pl.multiple_of(cols + j * lanes, lanes), lanes)
        tu, tg = taps_of(at_u), taps_of(at_g)
        vu = acc_s[:, at_u].astype(BF16).astype(F32)
        vg = acc_s[:, at_g].astype(BF16).astype(F32)
        cu, cg = conv(vu, tu, row), conv(vg, tg, row)
        sig = jax.nn.sigmoid(cg)
        upstream = cot[:, at_u].astype(F32)
        gu = upstream * (cg * sig)
        gg = upstream * cu * sig * (1.0 + cg * (1.0 - sig))
        gproj[:, at_u] = conv_back(gu, tu, row).astype(BF16)
        gproj[:, at_g] = conv_back(gg, tg, row).astype(BF16)
        for at, g, v in ((at_u, gu, vu), (at_g, gg, vg)):
            tloc[0:1, at] = jnp.sum(g * delayed(v, 2, row), axis=0, keepdims=True)
            tloc[1:2, at] = jnp.sum(g * delayed(v, 1, row), axis=0, keepdims=True)
            tloc[2:3, at] = jnp.sum(g * v, axis=0, keepdims=True)
        return carry

    lax.fori_loop(0, cols // lanes, backward, 0)

    def weight_term(b, size=1):
        rows_of = size * depth
        left = rows_s[:, pl.ds(pl.multiple_of(b * depth, rows_of), rows_of)].T
        step = tile_of(both)

        def body(j, carry):
            tile = pl.ds(pl.multiple_of(j * step, step), step)
            term = jnp.dot(left, gproj[:, tile], preferred_element_type=F32).astype(BF16)
            for i in range(size):
                gbuf[b + i, :, tile] = term[i * depth : (i + 1) * depth]
            return carry

        lax.fori_loop(0, both // step, body, 0)

    fars = [far_order(at, nz) for at in range(nz)]
    order = [pick(z, [o[q] for o in fars]) for q in range(nz)]

    def x_grad(b, d):
        to = lax.rem(x + d, nx)
        return remote(
            gbuf.at[b * nx + to], xrecv.at[d - 1, b], x_send.at[d - 1, b], x_recv.at[d - 1, b],
            z * nx + to, tp,
        )

    for q in range(nz):
        if whole:
            weight_term(order[q] * nx, size=nx)
        for d in range(1, nx):
            if not whole:
                weight_term(order[q] * nx + lax.rem(x + d, nx))
            x_grad(order[q], d).start()

    def tap_copy(d):
        return remote(
            tloc, trecv.at[d - 1], t_send.at[d - 1], t_recv.at[d - 1], lax.rem(me + d, nf), tp
        )

    for d in range(1, nf):
        tap_copy(d).start()

    def input_term(t):
        at = pl.ds(pl.multiple_of(t * part, part), part)
        step = tile_of(width)

        def body(j, carry):
            tile = pl.ds(pl.multiple_of(j * step, step), step)
            term = lax.dot_general(
                gproj[at, :], weights[tile, :], (((1,), (1,)), ((), ())), preferred_element_type=F32
            )
            pbuf[t, :, tile] = term.astype(BF16)
            return carry

        lax.fori_loop(0, width // step, body, 0)

    def part_copy(d):
        to = lax.rem(tp + d, nt)
        return remote(pbuf.at[to], precv.at[d - 1], p_send.at[d - 1], p_recv.at[d - 1], me, to)

    for d in range(1, nt):
        input_term(lax.rem(tp + d, nt))
        part_copy(d).start()
    for q in range(nz):
        if not whole:
            weight_term(order[q] * nx + x)
    input_term(tp)

    def forward(j, carry):
        row = lax.broadcasted_iota(jnp.int32, (seq, lanes), 0)
        at_u = pl.ds(pl.multiple_of(j * lanes, lanes), lanes)
        at_g = pl.ds(pl.multiple_of(cols + j * lanes, lanes), lanes)
        cu = conv(acc_l[:, at_u].astype(BF16).astype(F32), taps_of(at_u), row)
        cg = conv(acc_l[:, at_g].astype(BF16).astype(F32), taps_of(at_g), row)
        hidden_ref[:, at_u] = (cg * jax.nn.sigmoid(cg) * cu).astype(BF16)
        return carry

    lax.fori_loop(0, cols // lanes, forward, 0)

    total = tloc[...]
    for d in range(1, nf):
        tap_copy(d).wait_recv()
        total = total + trecv[d - 1]
    tapsum_ref[tp] = total

    def tap_full(d):
        return remote(
            tapsum_ref.at[tp], tapsum_ref.at[tp], tt_send.at[d - 1], tt_recv.at[tp],
            me, lax.rem(tp + d, nt),
        )

    for d in range(1, nt):
        tap_full(d).start()

    def add_into(b, sources):
        value = gbuf[b].astype(F32)
        for source in sources:
            value = value + source[...].astype(F32)
        gbuf[b] = value.astype(BF16)

    def up_grad(b):
        return remote(gbuf.at[b * nx + x], uprecv.at[b], up_send.at[b], up_recv.at[b], me + nx, tp)

    def dn_grad(b):
        return remote(gbuf.at[b * nx + x], dnrecv.at[b], dn_send.at[b], dn_recv.at[b], me - nx, tp)

    for q in range(nz):
        b = order[q]
        mine = b * nx + x
        for d in range(1, nx):
            x_grad(b, d).wait_recv()
        if q < nz - 1:
            fed = jnp.logical_or(jnp.logical_and(b > z, z > 0), jnp.logical_and(b < z, z < nz - 1))

            @pl.when(jnp.logical_and(b > z, z > 0))
            def _():
                up_grad(b).wait_recv()
                add_into(mine, [xrecv.at[d - 1, b] for d in range(1, nx)] + [uprecv.at[b]])

            @pl.when(jnp.logical_and(b < z, z < nz - 1))
            def _():
                dn_grad(b).wait_recv()
                add_into(mine, [xrecv.at[d - 1, b] for d in range(1, nx)] + [dnrecv.at[b]])

            @pl.when(jnp.logical_not(fed))
            def _():
                add_into(mine, [xrecv.at[d - 1, b] for d in range(1, nx)])

            @pl.when(b > z)
            def _():
                up_grad(b).start()

            @pl.when(b < z)
            def _():
                dn_grad(b).start()

        else:
            value = gbuf[mine].astype(F32)
            for d in range(1, nx):
                value = value + xrecv[d - 1, b].astype(F32)
            wsum_ref[...] = value

            @pl.when(z > 0)
            def _():
                up_grad(b).wait_recv()
                wsum_ref[...] += uprecv[b].astype(F32)

            @pl.when(z < nz - 1)
            def _():
                dn_grad(b).wait_recv()
                wsum_ref[...] += dnrecv[b].astype(F32)

    total = pbuf[tp].astype(F32)
    for d in range(1, nt):
        part_copy(d).wait_recv()
        total = total + precv[d - 1].astype(F32)
    ingrad_ref[...] = total.astype(BF16)

    for d in range(1, nt):
        remote(
            tapsum_ref.at[tp], tapsum_ref.at[lax.rem(tp + d, nt)], tt_send.at[d - 1],
            tt_recv.at[lax.rem(tp + d, nt)], me, lax.rem(tp + d, nt),
        ).wait_recv()
        tap_full(d).wait_send()
        part_copy(d).wait_send()
    for d in range(1, nf):
        tap_copy(d).wait_send()
    for copy in first_rows + forwards:
        copy.wait_send()
    for b in range(nz):
        for copy in x_copies(b):
            copy.wait_send()
        for d in range(1, nx):
            x_grad(b, d).wait_send()

        @pl.when(jnp.logical_and(z < nz - 1, b <= z))
        def _():
            up_copy(b).wait_send()

        @pl.when(jnp.logical_and(z > 0, b >= z))
        def _():
            dn_copy(b).wait_send()

        @pl.when(b > z)
        def _():
            up_grad(b).wait_send()

        @pl.when(b < z)
        def _():
            dn_grad(b).wait_send()


def shards(
    nf, nt,
    later_input, saved_input, cotangent, up_weight, gate_weight,
    up_taps, gate_taps, up_grad_sum, gate_grad_sum, up_taps_sum, gate_taps_sum,
):
    nx = 1 << ((nf.bit_length() - 1) // 2)
    nz = nf // nx
    depth, cols = up_weight.shape
    both = 2 * cols
    part, width = later_input.shape
    seq = part * nt
    tokens_all = part * nf * nt
    grad_scale = jnp.float32(tokens_all ** (-0.5))
    offset = lax.axis_index("tp") * cols
    taps_both = jnp.concatenate(
        [
            lax.dynamic_slice_in_dim(up_taps, offset, cols, 1),
            lax.dynamic_slice_in_dim(gate_taps, offset, cols, 1),
        ],
        axis=1,
    ).astype(F32)
    dma = pltpu.SemaphoreType.DMA
    vmem = pl.BlockSpec(memory_space=pltpu.VMEM)
    hbm = pl.BlockSpec(memory_space=pl.ANY)
    hidden, input_grad, weight_grad, taps_sum = pl.pallas_call(
        functools.partial(kernel, nx, nz, nt),
        out_shape=(
            jax.ShapeDtypeStruct((seq, cols), BF16),
            jax.ShapeDtypeStruct((part, width), BF16),
            jax.ShapeDtypeStruct((depth, both), F32),
            jax.ShapeDtypeStruct((nt, 8, both), F32),
        ),
        in_specs=[hbm] * 5 + [vmem],
        out_specs=(vmem,) * 4,
        scratch_shapes=[
            pltpu.VMEM((width, both), BF16),
            pltpu.VMEM((seq, width), BF16),
            pltpu.VMEM((seq, width), BF16),
            pltpu.VMEM((seq, cols), BF16),
            pltpu.VMEM((seq, both), F32),
            pltpu.VMEM((seq, both), F32),
            pltpu.VMEM((seq, both), BF16),
            pltpu.VMEM((nf, depth, both), BF16),
            pltpu.VMEM((nx - 1, nz, depth, both), BF16),
            pltpu.VMEM((nz, depth, both), BF16),
            pltpu.VMEM((nz, depth, both), BF16),
            pltpu.VMEM((nt, part, width), BF16),
            pltpu.VMEM((nt - 1, part, width), BF16),
            pltpu.VMEM((8, both), F32),
            pltpu.VMEM((nf - 1, 8, both), F32),
            dma((5,)),
            dma((nf,)),
            dma((nz,)),
            dma((nz,)),
            dma((nx - 1, nz)),
            dma((2, nt)),
            dma((2, nt)),
            dma((2, nt)),
            dma((nx - 1, nz)),
            dma((nx - 1, nz)),
            dma((nz,)),
            dma((nz,)),
            dma((nz,)),
            dma((nz,)),
            dma((nt - 1,)),
            dma((nt - 1,)),
            dma((nf - 1,)),
            dma((nf - 1,)),
            dma((nt - 1,)),
            dma((nt,)),
        ],
        compiler_params=pltpu.CompilerParams(
            collective_id=0, has_side_effects=True, vmem_limit_bytes=67043328
        ),
        name="layer",
    )(later_input, saved_input, cotangent, up_weight, gate_weight, taps_both)
    new_up_sum = up_grad_sum + grad_scale * weight_grad[:, :cols]
    new_gate_sum = gate_grad_sum + grad_scale * weight_grad[:, cols:]
    taps_up = taps_sum[:, :3, :cols].transpose(1, 0, 2).reshape(3, nt * cols)
    taps_gate = taps_sum[:, :3, cols:].transpose(1, 0, 2).reshape(3, nt * cols)
    new_up_taps_sum = up_taps_sum + grad_scale * taps_up
    new_gate_taps_sum = gate_taps_sum + grad_scale * taps_gate
    return (hidden, input_grad, new_up_sum, new_gate_sum, new_up_taps_sum, new_gate_taps_sum)


def solution(mesh):
    return jax.shard_map(
        functools.partial(shards, mesh.shape["fs"], mesh.shape["tp"]),
        mesh=mesh,
        in_specs=(
            P(("fs", "tp"), None),
            P(("fs", "tp"), None),
            P("fs", "tp"),
            P("fs", "tp"),
            P("fs", "tp"),
            P(),
            P(),
            P("fs", "tp"),
            P("fs", "tp"),
            P(),
            P(),
        ),
        out_specs=(P("fs", "tp"), P(("fs", "tp"), None), P("fs", "tp"), P("fs", "tp"), P(), P()),
        check_vma=False,
    )
```

```python
import functools

import jax
import jax.numpy as jnp
from jax import lax
from jax.experimental import pallas as pl
from jax.experimental.pallas import tpu as pltpu
from jax.sharding import PartitionSpec as P

MESH = pl.DeviceIdType.MESH
F32 = jnp.float32
BF16 = jnp.bfloat16
CORES = 2


def tile_of(extent):
    return 256 if extent % 256 == 0 else 128


def pick(index, table):
    value = jnp.int32(table[0])
    for at in range(1, len(table)):
        value = jnp.where(index == at, jnp.int32(table[at]), value)
    return value


def near_order(z, nz):
    order = [z]
    for step in range(1, nz):
        order += [b for b in (z - step, z + step) if 0 <= b < nz]
    return order


def far_order(z, nz):
    need = {b: (nz - 1 - b) + z if b > z else b + (nz - 1 - z) for b in range(nz) if b != z}
    return sorted(need, key=lambda b: (need[b], -abs(b - z))) + [z]


def delayed(values, steps, row):
    return jnp.where(row >= steps, pltpu.roll(values, steps, 0), 0.0)


def advanced(values, steps, row):
    extent = values.shape[0]
    return jnp.where(row < extent - steps, pltpu.roll(values, extent - steps, 0), 0.0)


def kernel(
    nx, nz, nt, scale,
    later_hbm, saved_hbm, cot_hbm, upw_hbm, gatew_hbm, upsum_hbm, gatesum_hbm,
    uptaps_ref, gatetaps_ref, uptsum_ref, gatetsum_ref,
    hidden_ref, ingrad_ref, newup_ref, newgate_ref, newupt_ref, newgatet_ref,
    weights, rows_l, rows_s, cot, acc_l, acc_s, gproj, gbuf, xrecv, uprecv, dnrecv,
    pbuf, precv, oldsum, taps, tloc, trecv, tzrecv, tapsum,
    local_sem, w_recv, w_up, w_dn, w_x, r_recv, r_send, r_fwd,
    x_send, x_recv, up_send, up_recv, dn_send, dn_recv, p_send, p_recv,
    t_send, t_recv, tz_send, tz_recv, tt_send, tt_recv,
):
    nf = nx * nz
    me = lax.axis_index("fs")
    tp = lax.axis_index("tp")
    x = lax.rem(me, nx)
    z = lax.div(me, nx)
    core = lax.rem(tp, CORES)
    chip = lax.div(tp, CORES)
    chips = nt // CORES
    depth = weights.shape[0] // nf
    both = weights.shape[1]
    cols = both // 2
    seq, width = rows_s.shape
    part = seq // nt

    def remote(src, dst, send, recv, f, t):
        return pltpu.make_async_remote_copy(
            src_ref=src, dst_ref=dst, send_sem=send, recv_sem=recv,
            device_id={"fs": f, "tp": t}, device_id_type=MESH,
        )

    def wblock(b):
        return weights.at[pl.ds(pl.multiple_of(b * depth, depth), depth), :]

    def rblock(ref, t):
        return ref.at[pl.ds(pl.multiple_of(t * part, part), part), :]

    own_w = [
        pltpu.make_async_copy(upw_hbm, wblock(me).at[:, pl.ds(0, cols)], local_sem.at[0]),
        pltpu.make_async_copy(gatew_hbm, wblock(me).at[:, pl.ds(cols, cols)], local_sem.at[1]),
    ]
    own_r = [
        pltpu.make_async_copy(saved_hbm, rblock(rows_s, tp), local_sem.at[2]),
        pltpu.make_async_copy(later_hbm, rblock(rows_l, tp), local_sem.at[3]),
    ]
    own_c = pltpu.make_async_copy(cot_hbm, cot, local_sem.at[4])
    own_s = [
        pltpu.make_async_copy(upsum_hbm, oldsum.at[0], local_sem.at[5]),
        pltpu.make_async_copy(gatesum_hbm, oldsum.at[1], local_sem.at[6]),
    ]
    for copy in own_w + own_r + [own_c] + own_s:
        copy.start()

    barrier = pltpu.get_barrier_semaphore()
    for d in range(1, nf):
        pl.semaphore_signal(
            barrier, inc=1, device_id={"fs": lax.rem(me + d, nf), "tp": tp}, device_id_type=MESH
        )
    for d in range(1, nt):
        pl.semaphore_signal(
            barrier, inc=1, device_id={"fs": me, "tp": lax.rem(tp + d, nt)}, device_id_type=MESH
        )
    pl.semaphore_wait(barrier, nf - 1 + nt - 1)

    def up_copy(b):
        return remote(wblock(b * nx + x), wblock(b * nx + x), w_up.at[b], w_recv.at[b * nx + x], me + nx, tp)

    def dn_copy(b):
        return remote(wblock(b * nx + x), wblock(b * nx + x), w_dn.at[b], w_recv.at[b * nx + x], me - nx, tp)

    def x_copies(b):
        return [
            remote(
                wblock(b * nx + x), wblock(b * nx + x), w_x.at[d - 1, b],
                w_recv.at[b * nx + x], z * nx + lax.rem(x + d, nx), tp,
            )
            for d in range(1, nx)
        ]

    def w_arrived(b):
        remote(wblock(b), wblock(b), w_up.at[0], w_recv.at[b], me, tp).wait_recv()

    for copy in own_w:
        copy.wait()

    @pl.when(z < nz - 1)
    def _():
        up_copy(z).start()

    @pl.when(z > 0)
    def _():
        dn_copy(z).start()

    for copy in x_copies(z):
        copy.start()

    for copy in own_r:
        copy.wait()
    rows = [rows_s, rows_l]
    mate = chip * CORES + (CORES - 1 - core)

    def row_copy(a, owner, target, sem):
        return remote(rblock(rows[a], owner), rblock(rows[a], owner), sem, r_recv.at[a, owner], me, target)

    def row_arrived(a, owner):
        row_copy(a, owner, tp, r_send.at[0, 0]).wait_recv()

    first_rows = []
    for a in range(2):
        for d in range(1, chips):
            target = lax.rem(chip + d, chips) * CORES + core
            first_rows.append(row_copy(a, tp, target, r_send.at[a, d]))
        first_rows.append(row_copy(a, tp, mate, r_send.at[a, 0]))
    for copy in first_rows:
        copy.start()

    whole = depth % 128 != 0

    def project(b, first=False, size=1):
        rows_of = size * depth
        at = pl.ds(pl.multiple_of(b * depth, rows_of), rows_of)
        step = tile_of(both)

        def body(j, carry):
            tile = pl.ds(pl.multiple_of(j * step, step), step)
            w = weights[at, tile]
            for r, acc in ((rows_s, acc_s), (rows_l, acc_l)):
                term = jnp.dot(r[:, at], w, preferred_element_type=F32)
                if first:
                    acc[:, tile] = term
                else:
                    acc[:, tile] += term
            return carry

        lax.fori_loop(0, both // step, body, 0)

    nears = [near_order(at, nz) for at in range(nz)]
    forwards = []
    for step in range(nz + 1):
        if 0 < step < nz:
            low, high = z - step, z + step

            @pl.when(low >= 0)
            def _():
                w_arrived(low * nx + x)

                @pl.when(z < nz - 1)
                def _():
                    up_copy(low).start()

                for copy in x_copies(low):
                    copy.start()

            @pl.when(high < nz)
            def _():
                w_arrived(high * nx + x)

                @pl.when(z > 0)
                def _():
                    dn_copy(high).start()

                for copy in x_copies(high):
                    copy.start()

        if step == 1:
            for a in range(2):
                for d in range(1, chips):
                    owner = lax.rem(chip + d, chips) * CORES + core
                    row_arrived(a, owner)
                    copy = row_copy(a, owner, mate, r_fwd.at[a, d])
                    copy.start()
                    forwards.append(copy)
            for a in range(2):
                for d in range(chips):
                    row_arrived(a, lax.rem(chip + d, chips) * CORES + (CORES - 1 - core))
            if not whole:
                project(me, first=True)
        if 0 < step < nz and not whole:

            @pl.when(low >= 0)
            def _():
                project(low * nx + x)

            @pl.when(high < nz)
            def _():
                project(high * nx + x)

        if step > 0:
            b = pick(z, [order[step - 1] for order in nears])
            for d in range(1, nx):
                block = b * nx + lax.rem(x + d, nx)
                w_arrived(block)
                if not whole:
                    project(block)
            if whole:
                project(b * nx, first=step == 1, size=nx)

    own_c.wait()
    lanes = 128

    tap_lanes = pl.ds(pl.multiple_of(tp * cols, 128), cols)
    taps[0:3, 0:cols] = uptaps_ref[:, tap_lanes].astype(F32)
    taps[0:3, cols:both] = gatetaps_ref[:, tap_lanes].astype(F32)

    def taps_of(at):
        return [taps[k : k + 1, at] for k in range(3)]

    def conv(values, taps, row):
        return taps[2] * values + taps[1] * delayed(values, 1, row) + taps[0] * delayed(values, 2, row)

    def conv_back(grads, taps, row):
        return taps[2] * grads + taps[1] * advanced(grads, 1, row) + taps[0] * advanced(grads, 2, row)

    tloc[...] = jnp.zeros_like(tloc)

    def backward(j, carry):
        row = lax.broadcasted_iota(jnp.int32, (seq, lanes), 0)
        at_u = pl.ds(pl.multiple_of(j * lanes, lanes), lanes)
        at_g = pl.ds(pl.multiple_of(cols + j * lanes, lanes), lanes)
        tu, tg = taps_of(at_u), taps_of(at_g)
        vu = acc_s[:, at_u].astype(BF16).astype(F32)
        vg = acc_s[:, at_g].astype(BF16).astype(F32)
        cu, cg = conv(vu, tu, row), conv(vg, tg, row)
        sig = jax.nn.sigmoid(cg)
        upstream = cot[:, at_u].astype(F32)
        gu = upstream * (cg * sig)
        gg = upstream * cu * sig * (1.0 + cg * (1.0 - sig))
        gproj[:, at_u] = conv_back(gu, tu, row).astype(BF16)
        gproj[:, at_g] = conv_back(gg, tg, row).astype(BF16)
        for k, g, v in ((0, gu, vu), (3, gg, vg)):
            tloc[k : k + 1, at_u] = jnp.sum(g * delayed(v, 2, row), axis=0, keepdims=True)
            tloc[k + 1 : k + 2, at_u] = jnp.sum(g * delayed(v, 1, row), axis=0, keepdims=True)
            tloc[k + 2 : k + 3, at_u] = jnp.sum(g * v, axis=0, keepdims=True)
        return carry

    lax.fori_loop(0, cols // lanes, backward, 0)

    def weight_term(b, size=1):
        rows_of = size * depth
        left = rows_s[:, pl.ds(pl.multiple_of(b * depth, rows_of), rows_of)].T
        step = tile_of(both)

        def body(j, carry):
            tile = pl.ds(pl.multiple_of(j * step, step), step)
            term = jnp.dot(left, gproj[:, tile], preferred_element_type=F32).astype(BF16)
            for i in range(size):
                gbuf[b + i, :, tile] = term[i * depth : (i + 1) * depth]
            return carry

        lax.fori_loop(0, both // step, body, 0)

    fars = [far_order(at, nz) for at in range(nz)]
    order = [pick(z, [o[q] for o in fars]) for q in range(nz)]

    def x_grad(b, d):
        to = lax.rem(x + d, nx)
        return remote(
            gbuf.at[b * nx + to], xrecv.at[d - 1, b], x_send.at[d - 1, b], x_recv.at[d - 1, b],
            z * nx + to, tp,
        )

    def tap_x(d):
        return remote(
            tloc, trecv.at[d - 1], t_send.at[d - 1], t_recv.at[d - 1], z * nx + lax.rem(x + d, nx), tp
        )

    for d in range(1, nx):
        tap_x(d).start()

    for q in range(nz):
        if whole:
            weight_term(order[q] * nx, size=nx)
        for d in range(1, nx):
            if not whole:
                weight_term(order[q] * nx + lax.rem(x + d, nx))
            x_grad(order[q], d).start()

    def input_term(t):
        at = pl.ds(pl.multiple_of(t * part, part), part)
        step = tile_of(width)

        def body(j, carry):
            tile = pl.ds(pl.multiple_of(j * step, step), step)
            term = lax.dot_general(
                gproj[at, :], weights[tile, :], (((1,), (1,)), ((), ())), preferred_element_type=F32
            )
            pbuf[t, :, tile] = term.astype(BF16)
            return carry

        lax.fori_loop(0, width // step, body, 0)

    def part_copy(d):
        to = lax.rem(tp + d, nt)
        return remote(pbuf.at[to], precv.at[d - 1], p_send.at[d - 1], p_recv.at[d - 1], me, to)

    for d in range(1, nt):
        input_term(lax.rem(tp + d, nt))
        part_copy(d).start()
    for q in range(nz):
        if not whole:
            weight_term(order[q] * nx + x)
    input_term(tp)

    def forward(j, carry):
        row = lax.broadcasted_iota(jnp.int32, (seq, lanes), 0)
        at_u = pl.ds(pl.multiple_of(j * lanes, lanes), lanes)
        at_g = pl.ds(pl.multiple_of(cols + j * lanes, lanes), lanes)
        cu = conv(acc_l[:, at_u].astype(BF16).astype(F32), taps_of(at_u), row)
        cg = conv(acc_l[:, at_g].astype(BF16).astype(F32), taps_of(at_g), row)
        hidden_ref[:, at_u] = (cg * jax.nn.sigmoid(cg) * cu).astype(BF16)
        return carry

    lax.fori_loop(0, cols // lanes, forward, 0)

    total = tloc[...]
    for d in range(1, nx):
        tap_x(d).wait_recv()
        total = total + trecv[d - 1]
    tzrecv[nz - 1] = total

    def tap_z(d):
        return remote(
            tzrecv.at[nz - 1], tzrecv.at[d - 1], tz_send.at[d - 1], tz_recv.at[d - 1],
            lax.rem(z + d, nz) * nx + x, tp,
        )

    def tap_full(d):
        return remote(
            tapsum.at[tp], tapsum.at[tp], tt_send.at[d - 1], tt_recv.at[tp], me, lax.rem(tp + d, nt)
        )

    for d in range(1, nz):
        tap_z(d).start()

    def add_into(b, sources):
        value = gbuf[b].astype(F32)
        for source in sources:
            value = value + source[...].astype(F32)
        gbuf[b] = value.astype(BF16)

    def up_grad(b):
        return remote(gbuf.at[b * nx + x], uprecv.at[b], up_send.at[b], up_recv.at[b], me + nx, tp)

    def dn_grad(b):
        return remote(gbuf.at[b * nx + x], dnrecv.at[b], dn_send.at[b], dn_recv.at[b], me - nx, tp)

    for q in range(nz):
        b = order[q]
        mine = b * nx + x
        for d in range(1, nx):
            x_grad(b, d).wait_recv()
        if q < nz - 1:
            fed = jnp.logical_or(jnp.logical_and(b > z, z > 0), jnp.logical_and(b < z, z < nz - 1))

            @pl.when(jnp.logical_and(b > z, z > 0))
            def _():
                up_grad(b).wait_recv()
                add_into(mine, [xrecv.at[d - 1, b] for d in range(1, nx)] + [uprecv.at[b]])

            @pl.when(jnp.logical_and(b < z, z < nz - 1))
            def _():
                dn_grad(b).wait_recv()
                add_into(mine, [xrecv.at[d - 1, b] for d in range(1, nx)] + [dnrecv.at[b]])

            @pl.when(jnp.logical_not(fed))
            def _():
                add_into(mine, [xrecv.at[d - 1, b] for d in range(1, nx)])

            @pl.when(b > z)
            def _():
                up_grad(b).start()

            @pl.when(b < z)
            def _():
                dn_grad(b).start()

        else:
            for copy in own_s:
                copy.wait()
            halves = ((newup_ref, 0, pl.ds(0, cols)), (newgate_ref, 1, pl.ds(cols, cols)))
            for new, at, lane in halves:
                value = gbuf[mine, :, lane].astype(F32)
                for d in range(1, nx):
                    value = value + xrecv[d - 1, b, :, lane].astype(F32)
                new[...] = oldsum[at] + scale * value

            @pl.when(z > 0)
            def _():
                up_grad(b).wait_recv()
                for new, at, lane in halves:
                    new[...] += scale * uprecv[b, :, lane].astype(F32)

            @pl.when(z < nz - 1)
            def _():
                dn_grad(b).wait_recv()
                for new, at, lane in halves:
                    new[...] += scale * dnrecv[b, :, lane].astype(F32)

        if q == 0:
            total = tzrecv[nz - 1]
            for d in range(1, nz):
                tap_z(d).wait_recv()
                total = total + tzrecv[d - 1]
            tapsum[tp] = total
            for d in range(1, nt):
                tap_full(d).start()

    total = pbuf[tp].astype(F32)
    for d in range(1, nt):
        part_copy(d).wait_recv()
        total = total + precv[d - 1].astype(F32)
    ingrad_ref[...] = total.astype(BF16)

    for d in range(1, nt):
        from_tp = lax.rem(tp + d, nt)
        remote(
            tapsum.at[tp], tapsum.at[from_tp], tt_send.at[d - 1], tt_recv.at[from_tp], me, from_tp
        ).wait_recv()
        tap_full(d).wait_send()
        part_copy(d).wait_send()
    for t in range(nt):
        lane = pl.ds(t * cols, cols)
        newupt_ref[:, lane] = uptsum_ref[:, lane] + scale * tapsum[t, 0:3]
        newgatet_ref[:, lane] = gatetsum_ref[:, lane] + scale * tapsum[t, 3:6]
    for d in range(1, nx):
        tap_x(d).wait_send()
    for d in range(1, nz):
        tap_z(d).wait_send()
    for copy in first_rows + forwards:
        copy.wait_send()
    for b in range(nz):
        for copy in x_copies(b):
            copy.wait_send()
        for d in range(1, nx):
            x_grad(b, d).wait_send()

        @pl.when(jnp.logical_and(z < nz - 1, b <= z))
        def _():
            up_copy(b).wait_send()

        @pl.when(jnp.logical_and(z > 0, b >= z))
        def _():
            dn_copy(b).wait_send()

        @pl.when(b > z)
        def _():
            up_grad(b).wait_send()

        @pl.when(b < z)
        def _():
            dn_grad(b).wait_send()


def shards(
    nf, nt,
    later_input, saved_input, cotangent, up_weight, gate_weight,
    up_taps, gate_taps, up_grad_sum, gate_grad_sum, up_taps_sum, gate_taps_sum,
):
    nx = 1 << ((nf.bit_length() - 1) // 2)
    nz = nf // nx
    depth, cols = up_weight.shape
    both = 2 * cols
    part, width = later_input.shape
    seq = part * nt
    scale = float(part * nf * nt) ** (-0.5)
    total_cols = up_taps.shape[1]
    dma = pltpu.SemaphoreType.DMA
    vmem = pl.BlockSpec(memory_space=pltpu.VMEM)
    hbm = pl.BlockSpec(memory_space=pl.ANY)
    return pl.pallas_call(
        functools.partial(kernel, nx, nz, nt, scale),
        out_shape=(
            jax.ShapeDtypeStruct((seq, cols), BF16),
            jax.ShapeDtypeStruct((part, width), BF16),
            jax.ShapeDtypeStruct((depth, cols), F32),
            jax.ShapeDtypeStruct((depth, cols), F32),
            jax.ShapeDtypeStruct((3, total_cols), F32),
            jax.ShapeDtypeStruct((3, total_cols), F32),
        ),
        in_specs=[hbm] * 7 + [vmem] * 4,
        out_specs=(vmem,) * 6,
        scratch_shapes=[
            pltpu.VMEM((width, both), BF16),
            pltpu.VMEM((seq, width), BF16),
            pltpu.VMEM((seq, width), BF16),
            pltpu.VMEM((seq, cols), BF16),
            pltpu.VMEM((seq, both), F32),
            pltpu.VMEM((seq, both), F32),
            pltpu.VMEM((seq, both), BF16),
            pltpu.VMEM((nf, depth, both), BF16),
            pltpu.VMEM((nx - 1, nz, depth, both), BF16),
            pltpu.VMEM((nz, depth, both), BF16),
            pltpu.VMEM((nz, depth, both), BF16),
            pltpu.VMEM((nt, part, width), BF16),
            pltpu.VMEM((nt - 1, part, width), BF16),
            pltpu.VMEM((2, depth, cols), F32),
            pltpu.VMEM((8, both), F32),
            pltpu.VMEM((8, cols), F32),
            pltpu.VMEM((nx - 1, 8, cols), F32),
            pltpu.VMEM((nz, 8, cols), F32),
            pltpu.VMEM((nt, 8, cols), F32),
            dma((7,)),
            dma((nf,)),
            dma((nz,)),
            dma((nz,)),
            dma((nx - 1, nz)),
            dma((2, nt)),
            dma((2, nt)),
            dma((2, nt)),
            dma((nx - 1, nz)),
            dma((nx - 1, nz)),
            dma((nz,)),
            dma((nz,)),
            dma((nz,)),
            dma((nz,)),
            dma((nt - 1,)),
            dma((nt - 1,)),
            dma((nx - 1,)),
            dma((nx - 1,)),
            dma((nz - 1,)),
            dma((nz - 1,)),
            dma((nt - 1,)),
            dma((nt,)),
        ],
        compiler_params=pltpu.CompilerParams(
            collective_id=0, has_side_effects=True, vmem_limit_bytes=67043328
        ),
        name="layer",
    )(
        later_input, saved_input, cotangent, up_weight, gate_weight, up_grad_sum, gate_grad_sum,
        up_taps, gate_taps, up_taps_sum, gate_taps_sum,
    )


def solution(mesh):
    return jax.shard_map(
        functools.partial(shards, mesh.shape["fs"], mesh.shape["tp"]),
        mesh=mesh,
        in_specs=(
            P(("fs", "tp"), None),
            P(("fs", "tp"), None),
            P("fs", "tp"),
            P("fs", "tp"),
            P("fs", "tp"),
            P(),
            P(),
            P("fs", "tp"),
            P("fs", "tp"),
            P(),
            P(),
        ),
        out_specs=(P("fs", "tp"), P(("fs", "tp"), None), P("fs", "tp"), P("fs", "tp"), P(), P()),
        check_vma=False,
    )
```

```python
import functools

import jax
import jax.numpy as jnp
from jax import lax
from jax.experimental import pallas as pl
from jax.experimental.pallas import tpu as pltpu
from jax.sharding import PartitionSpec as P

MESH = pl.DeviceIdType.MESH
F32 = jnp.float32
BF16 = jnp.bfloat16
CORES = 2


def tile_of(extent):
    return 256 if extent % 256 == 0 else 128


def pick(index, table):
    value = jnp.int32(table[0])
    for at in range(1, len(table)):
        value = jnp.where(index == at, jnp.int32(table[at]), value)
    return value


def near_order(z, nz):
    pair = z ^ 1
    order = [z]
    for step in range(1, nz):
        order += [b for b in (z - step, z + step) if 0 <= b < nz and b != pair]
    return order + [pair]


def far_order(z, nz):
    need = {b: (nz - 1 - b) + z if b > z else b + (nz - 1 - z) for b in range(nz) if b != z}
    return sorted(need, key=lambda b: (need[b], -abs(b - z))) + [z]


def delayed(values, steps, row):
    return jnp.where(row >= steps, pltpu.roll(values, steps, 0), 0.0)


def advanced(values, steps, row):
    extent = values.shape[0]
    return jnp.where(row < extent - steps, pltpu.roll(values, extent - steps, 0), 0.0)


def kernel(
    nx, nz, nt, scale,
    later_hbm, saved_hbm, cot_hbm, upw_hbm, gatew_hbm, upsum_hbm, gatesum_hbm,
    uptaps_ref, gatetaps_ref, uptsum_ref, gatetsum_ref,
    hidden_ref, ingrad_ref, newup_ref, newgate_ref, newupt_ref, newgatet_ref,
    weights, rows_l, rows_s, cot, acc_l, acc_s, gproj, gbuf, xrecv, uprecv, dnrecv,
    swrecv, pbuf, precv, oldsum, taps, tloc, trecv, tzrecv, tapsum,
    local_sem, w_recv, w_up, w_dn, w_x, w_swap, r_recv, r_send, r_fwd,
    x_send, x_recv, sw_send, sw_recv, up_send, up_recv, dn_send, dn_recv, p_send, p_recv,
    t_send, t_recv, tz_send, tz_recv, tt_send, tt_recv,
):
    nf = nx * nz
    me = lax.axis_index("fs")
    tp = lax.axis_index("tp")
    x = lax.rem(me, nx)
    z = lax.div(me, nx)
    core = lax.rem(tp, CORES)
    chip = lax.div(tp, CORES)
    chips = nt // CORES
    pair = z + 1 - 2 * lax.rem(z, 2)
    depth = weights.shape[0] // nf
    both = weights.shape[1]
    cols = both // 2
    seq, width = rows_s.shape
    part = seq // nt
    half = depth // 2

    def remote(src, dst, send, recv, f, t):
        return pltpu.make_async_remote_copy(
            src_ref=src, dst_ref=dst, send_sem=send, recv_sem=recv,
            device_id={"fs": f, "tp": t}, device_id_type=MESH,
        )

    def wblock(b):
        return weights.at[pl.ds(pl.multiple_of(b * depth, depth), depth), :]

    def rblock(ref, t):
        return ref.at[pl.ds(pl.multiple_of(t * part, part), part), :]

    own_w = [
        pltpu.make_async_copy(upw_hbm, wblock(me).at[:, pl.ds(0, cols)], local_sem.at[0]),
        pltpu.make_async_copy(gatew_hbm, wblock(me).at[:, pl.ds(cols, cols)], local_sem.at[1]),
    ]
    own_r = [
        pltpu.make_async_copy(saved_hbm, rblock(rows_s, tp), local_sem.at[2]),
        pltpu.make_async_copy(later_hbm, rblock(rows_l, tp), local_sem.at[3]),
    ]
    own_c = pltpu.make_async_copy(cot_hbm, cot, local_sem.at[4])
    own_s = [
        pltpu.make_async_copy(upsum_hbm, oldsum.at[0], local_sem.at[5]),
        pltpu.make_async_copy(gatesum_hbm, oldsum.at[1], local_sem.at[6]),
    ]
    for copy in own_w + own_r + [own_c] + own_s:
        copy.start()

    barrier = pltpu.get_barrier_semaphore()
    for d in range(1, nf):
        pl.semaphore_signal(
            barrier, inc=1, device_id={"fs": lax.rem(me + d, nf), "tp": tp}, device_id_type=MESH
        )
    for d in range(1, nt):
        pl.semaphore_signal(
            barrier, inc=1, device_id={"fs": me, "tp": lax.rem(tp + d, nt)}, device_id_type=MESH
        )
    pl.semaphore_wait(barrier, nf - 1 + nt - 1)

    def whalf(b, i):
        return weights.at[pl.ds(pl.multiple_of(b * depth + i * half, half), half), :]

    def w_copy(b, i, send, f):
        return remote(whalf(b, i), whalf(b, i), send, w_recv.at[b, i], f, tp)

    def up_copy(b, i):
        return w_copy(b * nx + x, i, w_up.at[b, i], me + nx)

    def dn_copy(b, i):
        return w_copy(b * nx + x, i, w_dn.at[b, i], me - nx)

    def x_copies(b, i):
        return [
            w_copy(b * nx + x, i, w_x.at[d - 1, b, i], z * nx + lax.rem(x + d, nx))
            for d in range(1, nx)
        ]

    def swap_copy(d):
        return w_copy(z * nx + lax.rem(x + d, nx), 1, w_swap.at[d - 1], pair * nx + x)

    def pass_x(b, i):
        if i == 0:
            for copy in x_copies(b, i):
                copy.start()
        else:

            @pl.when(b != pair)
            def _():
                for copy in x_copies(b, i):
                    copy.start()

    def w_arrived(b, i):
        w_copy(b, i, w_up.at[0, 0], me).wait_recv()

    for copy in own_w:
        copy.wait()

    for i in range(2):

        @pl.when(z < nz - 1)
        def _():
            up_copy(z, i).start()

        @pl.when(z > 0)
        def _():
            dn_copy(z, i).start()

        for copy in x_copies(z, i):
            copy.start()

    for copy in own_r:
        copy.wait()
    rows = [rows_s, rows_l]
    mate = chip * CORES + (CORES - 1 - core)

    def row_copy(a, owner, target, sem):
        return remote(rblock(rows[a], owner), rblock(rows[a], owner), sem, r_recv.at[a, owner], me, target)

    def row_arrived(a, owner):
        row_copy(a, owner, tp, r_send.at[0, 0]).wait_recv()

    first_rows = []
    for a in range(2):
        for d in range(1, chips):
            target = lax.rem(chip + d, chips) * CORES + core
            first_rows.append(row_copy(a, tp, target, r_send.at[a, d]))
        first_rows.append(row_copy(a, tp, mate, r_send.at[a, 0]))
    for copy in first_rows:
        copy.start()

    whole = depth % 128 != 0

    def project(b, first=False, size=1, which=(0, 1)):
        rows_of = size * depth
        at = pl.ds(pl.multiple_of(b * depth, rows_of), rows_of)
        step = tile_of(both)

        def body(j, carry):
            tile = pl.ds(pl.multiple_of(j * step, step), step)
            w = weights[at, tile]
            for a in which:
                r, acc = ((rows_s, acc_s), (rows_l, acc_l))[a]
                term = jnp.dot(r[:, at], w, preferred_element_type=F32)
                if first:
                    acc[:, tile] = term
                else:
                    acc[:, tile] += term
            return carry

        lax.fori_loop(0, both // step, body, 0)

    nears = [near_order(at, nz) for at in range(nz)]
    forwards = []
    for step in range(nz + 1):
        if 0 < step < nz:
            low, high = z - step, z + step

            for i in range(2):

                @pl.when(low >= 0)
                def _():
                    w_arrived(low * nx + x, i)

                    @pl.when(z < nz - 1)
                    def _():
                        up_copy(low, i).start()

                    pass_x(low, i)

                @pl.when(high < nz)
                def _():
                    w_arrived(high * nx + x, i)

                    @pl.when(z > 0)
                    def _():
                        dn_copy(high, i).start()

                    pass_x(high, i)

        if step == 1:
            for a in range(2):
                for d in range(1, chips):
                    owner = lax.rem(chip + d, chips) * CORES + core
                    row_arrived(a, owner)
                    copy = row_copy(a, owner, mate, r_fwd.at[a, d])
                    copy.start()
                    forwards.append(copy)
            for a in range(2):
                for d in range(chips):
                    row_arrived(a, lax.rem(chip + d, chips) * CORES + (CORES - 1 - core))
            if not whole:
                project(me, first=True)
        if 0 < step < nz and not whole:

            @pl.when(low >= 0)
            def _():
                project(low * nx + x)

            @pl.when(high < nz)
            def _():
                project(high * nx + x)

        if step > 0:
            b = pick(z, [order[step - 1] for order in nears])
            which = (0, 1) if step < nz - 1 else (0,)
            for d in range(1, nx):
                block = b * nx + lax.rem(x + d, nx)
                for i in range(2):
                    w_arrived(block, i)
                if not whole:
                    project(block, which=which)
            if whole:
                project(b * nx, first=step == 1, size=nx, which=which)
        if step == nz - 2:
            for d in range(1, nx):
                swap_copy(d).start()

    own_c.wait()
    lanes = 128

    tap_lanes = pl.ds(pl.multiple_of(tp * cols, 128), cols)
    taps[0:3, 0:cols] = uptaps_ref[:, tap_lanes].astype(F32)
    taps[0:3, cols:both] = gatetaps_ref[:, tap_lanes].astype(F32)

    def taps_of(at):
        return [taps[k : k + 1, at] for k in range(3)]

    def conv(values, taps, row):
        return taps[2] * values + taps[1] * delayed(values, 1, row) + taps[0] * delayed(values, 2, row)

    def conv_back(grads, taps, row):
        return taps[2] * grads + taps[1] * advanced(grads, 1, row) + taps[0] * advanced(grads, 2, row)

    tloc[...] = jnp.zeros_like(tloc)

    def backward(j, carry):
        row = lax.broadcasted_iota(jnp.int32, (seq, lanes), 0)
        at_u = pl.ds(pl.multiple_of(j * lanes, lanes), lanes)
        at_g = pl.ds(pl.multiple_of(cols + j * lanes, lanes), lanes)
        tu, tg = taps_of(at_u), taps_of(at_g)
        vu = acc_s[:, at_u].astype(BF16).astype(F32)
        vg = acc_s[:, at_g].astype(BF16).astype(F32)
        cu, cg = conv(vu, tu, row), conv(vg, tg, row)
        sig = jax.nn.sigmoid(cg)
        upstream = cot[:, at_u].astype(F32)
        gu = upstream * (cg * sig)
        gg = upstream * cu * sig * (1.0 + cg * (1.0 - sig))
        gproj[:, at_u] = conv_back(gu, tu, row).astype(BF16)
        gproj[:, at_g] = conv_back(gg, tg, row).astype(BF16)
        for k, g, v in ((0, gu, vu), (3, gg, vg)):
            tloc[k : k + 1, at_u] = jnp.sum(g * delayed(v, 2, row), axis=0, keepdims=True)
            tloc[k + 1 : k + 2, at_u] = jnp.sum(g * delayed(v, 1, row), axis=0, keepdims=True)
            tloc[k + 2 : k + 3, at_u] = jnp.sum(g * v, axis=0, keepdims=True)
        return carry

    lax.fori_loop(0, cols // lanes, backward, 0)

    def weight_term(b, size=1):
        rows_of = size * depth
        left = rows_s[:, pl.ds(pl.multiple_of(b * depth, rows_of), rows_of)].T
        step = tile_of(both)

        def body(j, carry):
            tile = pl.ds(pl.multiple_of(j * step, step), step)
            term = jnp.dot(left, gproj[:, tile], preferred_element_type=F32).astype(BF16)
            for i in range(size):
                gbuf[b + i, :, tile] = term[i * depth : (i + 1) * depth]
            return carry

        lax.fori_loop(0, both // step, body, 0)

    fars = [far_order(at, nz) for at in range(nz)]
    order = [pick(z, [o[q] for o in fars]) for q in range(nz)]

    def hrows(i):
        return pl.ds(i * half, half)

    def x_grad(b, d, i):
        to = lax.rem(x + d, nx)
        return remote(
            gbuf.at[b * nx + to, hrows(i), :], xrecv.at[d - 1, b, hrows(i), :],
            x_send.at[d - 1, b, i], x_recv.at[d - 1, b, i], z * nx + to, tp,
        )

    def swap_grad(d):
        return remote(
            gbuf.at[pair * nx + lax.rem(x + d, nx), hrows(1), :], swrecv.at[d - 1],
            sw_send.at[d - 1], sw_recv.at[d - 1], pair * nx + x, tp,
        )

    def terms_of(b):
        if whole:
            weight_term(b * nx, size=nx)
        else:
            for d in range(1, nx):
                weight_term(b * nx + lax.rem(x + d, nx))

    def tap_x(d):
        return remote(
            tloc, trecv.at[d - 1], t_send.at[d - 1], t_recv.at[d - 1], z * nx + lax.rem(x + d, nx), tp
        )

    for d in range(1, nx):
        tap_x(d).start()

    for q in range(nz):
        b = order[q]
        if q == 0:
            terms_of(b)
        else:

            @pl.when(b != pair)
            def _():
                terms_of(b)

        for d in range(1, nx):
            x_grad(b, d, 0).start()

            if q < nz - 1:

                @pl.when(b != pair)
                def _():
                    x_grad(b, d, 1).start()

        if q == 0:
            terms_of(pair)
            for d in range(1, nx):
                swap_grad(d).start()
    for q in range(nz):
        if not whole:
            weight_term(order[q] * nx + x)

    def input_term(t):
        at = pl.ds(pl.multiple_of(t * part, part), part)
        step = tile_of(width)

        def body(j, carry):
            tile = pl.ds(pl.multiple_of(j * step, step), step)
            term = lax.dot_general(
                gproj[at, :], weights[tile, :], (((1,), (1,)), ((), ())), preferred_element_type=F32
            )
            pbuf[t, :, tile] = term.astype(BF16)
            return carry

        lax.fori_loop(0, width // step, body, 0)

    def part_copy(d):
        to = lax.rem(tp + d, nt)
        return remote(pbuf.at[to], precv.at[d - 1], p_send.at[d - 1], p_recv.at[d - 1], me, to)

    def all_input_terms():
        for d in range(1, nt):
            input_term(lax.rem(tp + d, nt))
            part_copy(d).start()
        input_term(tp)

    def forward(j, carry):
        row = lax.broadcasted_iota(jnp.int32, (seq, lanes), 0)
        at_u = pl.ds(pl.multiple_of(j * lanes, lanes), lanes)
        at_g = pl.ds(pl.multiple_of(cols + j * lanes, lanes), lanes)
        cu = conv(acc_l[:, at_u].astype(BF16).astype(F32), taps_of(at_u), row)
        cg = conv(acc_l[:, at_g].astype(BF16).astype(F32), taps_of(at_g), row)
        hidden_ref[:, at_u] = (cg * jax.nn.sigmoid(cg) * cu).astype(BF16)
        return carry

    def all_hidden():
        for at in range(nz - 2, nz):
            b = pick(z, [order[at] for order in nears])
            if whole:
                project(b * nx, size=nx, which=(1,))
            else:
                for d in range(1, nx):
                    project(b * nx + lax.rem(x + d, nx), which=(1,))
        lax.fori_loop(0, cols // lanes, forward, 0)

    total = tloc[...]
    for d in range(1, nx):
        tap_x(d).wait_recv()
        total = total + trecv[d - 1]
    tzrecv[nz - 1] = total

    def tap_z(d):
        return remote(
            tzrecv.at[nz - 1], tzrecv.at[d - 1], tz_send.at[d - 1], tz_recv.at[d - 1],
            lax.rem(z + d, nz) * nx + x, tp,
        )

    def tap_full(d):
        return remote(
            tapsum.at[tp], tapsum.at[tp], tt_send.at[d - 1], tt_recv.at[tp], me, lax.rem(tp + d, nt)
        )

    for d in range(1, nz):
        tap_z(d).start()

    def add_into(b, i, sources):
        value = gbuf[b, hrows(i), :].astype(F32)
        for source in sources:
            value = value + source[...].astype(F32)
        gbuf[b, hrows(i), :] = value.astype(BF16)

    def up_grad(b, i):
        return remote(
            gbuf.at[b * nx + x, hrows(i), :], uprecv.at[b, hrows(i), :],
            up_send.at[b, i], up_recv.at[b, i], me + nx, tp,
        )

    def dn_grad(b, i):
        return remote(
            gbuf.at[b * nx + x, hrows(i), :], dnrecv.at[b, hrows(i), :],
            dn_send.at[b, i], dn_recv.at[b, i], me - nx, tp,
        )

    for q in range(nz):
        b = order[q]
        mine = b * nx + x
        for i in range(2):
            if q < nz - 1:

                def from_x():
                    for d in range(1, nx):
                        x_grad(b, d, i).wait_recv()
                    add_into(mine, i, [xrecv.at[d - 1, b, hrows(i), :] for d in range(1, nx)])

                if i == 0:
                    from_x()
                else:
                    pl.when(b != pair)(from_x)

                @pl.when(b > z)
                def _():
                    @pl.when(z > 0)
                    def _():
                        up_grad(b, i).wait_recv()
                        add_into(mine, i, [uprecv.at[b, hrows(i), :]])

                    up_grad(b, i).start()

                @pl.when(b < z)
                def _():
                    @pl.when(z < nz - 1)
                    def _():
                        dn_grad(b, i).wait_recv()
                        add_into(mine, i, [dnrecv.at[b, hrows(i), :]])

                    dn_grad(b, i).start()

                continue
            if i == 0:
                for copy in own_s:
                    copy.wait()
            sides = ((newup_ref, 0, pl.ds(0, cols)), (newgate_ref, 1, pl.ds(cols, cols)))
            for d in range(1, nx):
                x_grad(b, d, i).wait_recv()
            for new, at, lane in sides:
                value = gbuf[mine, hrows(i), lane].astype(F32)
                for d in range(1, nx):
                    value = value + xrecv[d - 1, b, hrows(i), lane].astype(F32)
                new[hrows(i), :] = oldsum[at, hrows(i), :] + scale * value

            @pl.when(z > 0)
            def _():
                up_grad(b, i).wait_recv()
                for new, at, lane in sides:
                    new[hrows(i), :] += scale * uprecv[b, hrows(i), lane].astype(F32)

            @pl.when(z < nz - 1)
            def _():
                dn_grad(b, i).wait_recv()
                for new, at, lane in sides:
                    new[hrows(i), :] += scale * dnrecv[b, hrows(i), lane].astype(F32)

        if q == 0:
            for d in range(1, nx):
                swap_grad(d).wait_recv()
                add_into(z * nx + lax.rem(x + d, nx), 1, [swrecv.at[d - 1]])
                x_grad(z, d, 1).start()
            all_input_terms()
        if q == 1:
            all_hidden()
        if q == 0:
            total = tzrecv[nz - 1]
            for d in range(1, nz):
                tap_z(d).wait_recv()
                total = total + tzrecv[d - 1]
            tapsum[tp] = total
            for d in range(1, nt):
                tap_full(d).start()

    total = pbuf[tp].astype(F32)
    for d in range(1, nt):
        part_copy(d).wait_recv()
        total = total + precv[d - 1].astype(F32)
    ingrad_ref[...] = total.astype(BF16)

    for d in range(1, nt):
        from_tp = lax.rem(tp + d, nt)
        remote(
            tapsum.at[tp], tapsum.at[from_tp], tt_send.at[d - 1], tt_recv.at[from_tp], me, from_tp
        ).wait_recv()
        tap_full(d).wait_send()
        part_copy(d).wait_send()
    for t in range(nt):
        lane = pl.ds(t * cols, cols)
        newupt_ref[:, lane] = uptsum_ref[:, lane] + scale * tapsum[t, 0:3]
        newgatet_ref[:, lane] = gatetsum_ref[:, lane] + scale * tapsum[t, 3:6]
    for d in range(1, nx):
        tap_x(d).wait_send()
    for d in range(1, nz):
        tap_z(d).wait_send()
    for copy in first_rows + forwards:
        copy.wait_send()
    for d in range(1, nx):
        swap_copy(d).wait_send()
        swap_grad(d).wait_send()
    for b in range(nz):
        for i in range(2):

            def x_left():
                for copy in x_copies(b, i):
                    copy.wait_send()
                for d in range(1, nx):
                    x_grad(b, d, i).wait_send()

            if i == 0:
                x_left()
            else:
                pl.when(b != pair)(x_left)

            @pl.when(jnp.logical_and(z < nz - 1, b <= z))
            def _():
                up_copy(b, i).wait_send()

            @pl.when(jnp.logical_and(z > 0, b >= z))
            def _():
                dn_copy(b, i).wait_send()

            @pl.when(b > z)
            def _():
                up_grad(b, i).wait_send()

            @pl.when(b < z)
            def _():
                dn_grad(b, i).wait_send()


def shards(
    nf, nt,
    later_input, saved_input, cotangent, up_weight, gate_weight,
    up_taps, gate_taps, up_grad_sum, gate_grad_sum, up_taps_sum, gate_taps_sum,
):
    nx = 1 << ((nf.bit_length() - 1) // 2)
    nz = nf // nx
    depth, cols = up_weight.shape
    both = 2 * cols
    part, width = later_input.shape
    seq = part * nt
    scale = float(part * nf * nt) ** (-0.5)
    total_cols = up_taps.shape[1]
    dma = pltpu.SemaphoreType.DMA
    vmem = pl.BlockSpec(memory_space=pltpu.VMEM)
    hbm = pl.BlockSpec(memory_space=pl.ANY)
    return pl.pallas_call(
        functools.partial(kernel, nx, nz, nt, scale),
        out_shape=(
            jax.ShapeDtypeStruct((seq, cols), BF16),
            jax.ShapeDtypeStruct((part, width), BF16),
            jax.ShapeDtypeStruct((depth, cols), F32),
            jax.ShapeDtypeStruct((depth, cols), F32),
            jax.ShapeDtypeStruct((3, total_cols), F32),
            jax.ShapeDtypeStruct((3, total_cols), F32),
        ),
        in_specs=[hbm] * 7 + [vmem] * 4,
        out_specs=(vmem,) * 6,
        scratch_shapes=[
            pltpu.VMEM((width, both), BF16),
            pltpu.VMEM((seq, width), BF16),
            pltpu.VMEM((seq, width), BF16),
            pltpu.VMEM((seq, cols), BF16),
            pltpu.VMEM((seq, both), F32),
            pltpu.VMEM((seq, both), F32),
            pltpu.VMEM((seq, both), BF16),
            pltpu.VMEM((nf, depth, both), BF16),
            pltpu.VMEM((nx - 1, nz, depth, both), BF16),
            pltpu.VMEM((nz, depth, both), BF16),
            pltpu.VMEM((nz, depth, both), BF16),
            pltpu.VMEM((nx - 1, depth // 2, both), BF16),
            pltpu.VMEM((nt, part, width), BF16),
            pltpu.VMEM((nt - 1, part, width), BF16),
            pltpu.VMEM((2, depth, cols), F32),
            pltpu.VMEM((8, both), F32),
            pltpu.VMEM((8, cols), F32),
            pltpu.VMEM((nx - 1, 8, cols), F32),
            pltpu.VMEM((nz, 8, cols), F32),
            pltpu.VMEM((nt, 8, cols), F32),
            dma((7,)),
            dma((nf, 2)),
            dma((nz, 2)),
            dma((nz, 2)),
            dma((nx - 1, nz, 2)),
            dma((nx - 1,)),
            dma((2, nt)),
            dma((2, nt)),
            dma((2, nt)),
            dma((nx - 1, nz, 2)),
            dma((nx - 1, nz, 2)),
            dma((nx - 1,)),
            dma((nx - 1,)),
            dma((nz, 2)),
            dma((nz, 2)),
            dma((nz, 2)),
            dma((nz, 2)),
            dma((nt - 1,)),
            dma((nt - 1,)),
            dma((nx - 1,)),
            dma((nx - 1,)),
            dma((nz - 1,)),
            dma((nz - 1,)),
            dma((nt - 1,)),
            dma((nt,)),
        ],
        compiler_params=pltpu.CompilerParams(
            collective_id=0, has_side_effects=True, vmem_limit_bytes=67043328
        ),
        name="layer",
    )(
        later_input, saved_input, cotangent, up_weight, gate_weight, up_grad_sum, gate_grad_sum,
        up_taps, gate_taps, up_taps_sum, gate_taps_sum,
    )


def solution(mesh):
    return jax.shard_map(
        functools.partial(shards, mesh.shape["fs"], mesh.shape["tp"]),
        mesh=mesh,
        in_specs=(
            P(("fs", "tp"), None),
            P(("fs", "tp"), None),
            P("fs", "tp"),
            P("fs", "tp"),
            P("fs", "tp"),
            P(),
            P(),
            P("fs", "tp"),
            P("fs", "tp"),
            P(),
            P(),
        ),
        out_specs=(P("fs", "tp"), P(("fs", "tp"), None), P("fs", "tp"), P("fs", "tp"), P(), P()),
        check_vma=False,
    )
```

```python
import functools

import jax
import jax.numpy as jnp
from jax import lax
from jax.experimental import pallas as pl
from jax.experimental.pallas import tpu as pltpu
from jax.sharding import PartitionSpec as P

MESH = pl.DeviceIdType.MESH
F32 = jnp.float32
BF16 = jnp.bfloat16
CORES = 2


def tile_of(extent):
    return 256 if extent % 256 == 0 else 128


def pick(index, table):
    value = jnp.int32(table[0])
    for at in range(1, len(table)):
        value = jnp.where(index == at, jnp.int32(table[at]), value)
    return value


def near_order(z, nz):
    pair = z ^ 1
    order = [z]
    for step in range(1, nz):
        order += [b for b in (z - step, z + step) if 0 <= b < nz and b != pair]
    return order + [pair]


def far_order(z, nz):
    need = {b: (nz - 1 - b) + z if b > z else b + (nz - 1 - z) for b in range(nz) if b != z}
    return sorted(need, key=lambda b: (need[b], -abs(b - z))) + [z]


def delayed(values, steps, row):
    return jnp.where(row >= steps, pltpu.roll(values, steps, 0), 0.0)


def advanced(values, steps, row):
    extent = values.shape[0]
    return jnp.where(row < extent - steps, pltpu.roll(values, extent - steps, 0), 0.0)


def kernel(
    nx, nz, nt, scale,
    later_hbm, saved_hbm, cot_hbm, upw_hbm, gatew_hbm, upsum_hbm, gatesum_hbm,
    uptaps_ref, gatetaps_ref, uptsum_ref, gatetsum_ref,
    hidden_ref, ingrad_ref, newup_ref, newgate_ref, newupt_ref, newgatet_ref,
    weights, rows_l, rows_s, cot, acc_l, acc_s, gproj, gbuf, xrecv, uprecv, dnrecv,
    swrecv, pbuf, precv, oldsum, taps, tloc, trecv, tzrecv, tapsum,
    local_sem, w_recv, w_up, w_dn, w_x, w_swap, r_recv, r_send, r_fwd,
    x_send, x_recv, sw_send, sw_recv, up_send, up_recv, dn_send, dn_recv, p_send, p_recv,
    t_send, t_recv, tz_send, tz_recv, tt_send, tt_recv,
):
    nf = nx * nz
    me = lax.axis_index("fs")
    tp = lax.axis_index("tp")
    x = lax.rem(me, nx)
    z = lax.div(me, nx)
    core = lax.rem(tp, CORES)
    chip = lax.div(tp, CORES)
    chips = nt // CORES
    pair = z + 1 - 2 * lax.rem(z, 2)
    depth = weights.shape[0] // nf
    both = weights.shape[1]
    cols = both // 2
    seq, width = rows_s.shape
    part = seq // nt
    half = depth // 2

    def remote(src, dst, send, recv, f, t):
        return pltpu.make_async_remote_copy(
            src_ref=src, dst_ref=dst, send_sem=send, recv_sem=recv,
            device_id={"fs": f, "tp": t}, device_id_type=MESH,
        )

    def wblock(b):
        return weights.at[pl.ds(pl.multiple_of(b * depth, depth), depth), :]

    def rblock(ref, t):
        return ref.at[pl.ds(pl.multiple_of(t * part, part), part), :]

    own_w = [
        pltpu.make_async_copy(upw_hbm, wblock(me).at[:, pl.ds(0, cols)], local_sem.at[0]),
        pltpu.make_async_copy(gatew_hbm, wblock(me).at[:, pl.ds(cols, cols)], local_sem.at[1]),
    ]
    own_r = [
        pltpu.make_async_copy(saved_hbm, rblock(rows_s, tp), local_sem.at[2]),
        pltpu.make_async_copy(later_hbm, rblock(rows_l, tp), local_sem.at[3]),
    ]
    own_c = pltpu.make_async_copy(cot_hbm, cot, local_sem.at[4])
    own_s = [
        pltpu.make_async_copy(upsum_hbm, oldsum.at[0], local_sem.at[5]),
        pltpu.make_async_copy(gatesum_hbm, oldsum.at[1], local_sem.at[6]),
    ]
    for copy in own_w + own_r + [own_c] + own_s:
        copy.start()

    barrier = pltpu.get_barrier_semaphore()
    for d in range(1, nf):
        pl.semaphore_signal(
            barrier, inc=1, device_id={"fs": lax.rem(me + d, nf), "tp": tp}, device_id_type=MESH
        )
    for d in range(1, nt):
        pl.semaphore_signal(
            barrier, inc=1, device_id={"fs": me, "tp": lax.rem(tp + d, nt)}, device_id_type=MESH
        )
    pl.semaphore_wait(barrier, nf - 1 + nt - 1)

    def whalf(b, i):
        return weights.at[pl.ds(pl.multiple_of(b * depth + i * half, half), half), :]

    def w_copy(b, i, send, f):
        return remote(whalf(b, i), whalf(b, i), send, w_recv.at[b, i], f, tp)

    def up_copy(b, i):
        return w_copy(b * nx + x, i, w_up.at[b, i], me + nx)

    def dn_copy(b, i):
        return w_copy(b * nx + x, i, w_dn.at[b, i], me - nx)

    def x_copies(b, i):
        return [
            w_copy(b * nx + x, i, w_x.at[d - 1, b, i], z * nx + lax.rem(x + d, nx))
            for d in range(1, nx)
        ]

    def swap_copy(d):
        return w_copy(z * nx + lax.rem(x + d, nx), 1, w_swap.at[d - 1], pair * nx + x)

    def pass_x(b, i):
        if i == 0:
            for copy in x_copies(b, i):
                copy.start()
        else:

            @pl.when(b != pair)
            def _():
                for copy in x_copies(b, i):
                    copy.start()

    def w_arrived(b, i):
        w_copy(b, i, w_up.at[0, 0], me).wait_recv()

    for copy in own_w:
        copy.wait()

    for i in range(2):

        @pl.when(z < nz - 1)
        def _():
            up_copy(z, i).start()

        @pl.when(z > 0)
        def _():
            dn_copy(z, i).start()

        for copy in x_copies(z, i):
            copy.start()

    for copy in own_r:
        copy.wait()
    rows = [rows_s, rows_l]
    mate = chip * CORES + (CORES - 1 - core)

    def row_copy(a, owner, target, sem):
        return remote(rblock(rows[a], owner), rblock(rows[a], owner), sem, r_recv.at[a, owner], me, target)

    def row_arrived(a, owner):
        row_copy(a, owner, tp, r_send.at[0, 0]).wait_recv()

    first_rows = []
    for a in range(2):
        for d in range(1, chips):
            target = lax.rem(chip + d, chips) * CORES + core
            first_rows.append(row_copy(a, tp, target, r_send.at[a, d]))
        first_rows.append(row_copy(a, tp, mate, r_send.at[a, 0]))
    for copy in first_rows:
        copy.start()

    whole = depth % 128 != 0

    def project(b, first=False, size=1, which=(0, 1)):
        rows_of = size * depth
        at = pl.ds(pl.multiple_of(b * depth, rows_of), rows_of)
        step = tile_of(both)

        def body(j, carry):
            tile = pl.ds(pl.multiple_of(j * step, step), step)
            w = weights[at, tile]
            for a in which:
                r, acc = ((rows_s, acc_s), (rows_l, acc_l))[a]
                term = jnp.dot(r[:, at], w, preferred_element_type=F32)
                if first:
                    acc[:, tile] = term
                else:
                    acc[:, tile] += term
            return carry

        lax.fori_loop(0, both // step, body, 0)

    nears = [near_order(at, nz) for at in range(nz)]
    forwards = []
    def pass_rows(a):
        for d in range(1, chips):
            owner = lax.rem(chip + d, chips) * CORES + core
            row_arrived(a, owner)
            copy = row_copy(a, owner, mate, r_fwd.at[a, d])
            copy.start()
            forwards.append(copy)

    def pass_z(step, i):
        low, high = z - step, z + step

        @pl.when(low >= 0)
        def _():
            w_arrived(low * nx + x, i)

            @pl.when(z < nz - 1)
            def _():
                up_copy(low, i).start()

            pass_x(low, i)

        @pl.when(high < nz)
        def _():
            w_arrived(high * nx + x, i)

            @pl.when(z > 0)
            def _():
                dn_copy(high, i).start()

            pass_x(high, i)

    def project_z(step):
        if not whole:
            low, high = z - step, z + step

            @pl.when(low >= 0)
            def _():
                project(low * nx + x)

            @pl.when(high < nz)
            def _():
                project(high * nx + x)

    def from_x(at):
        b = pick(z, [order[at] for order in nears])
        which = (0, 1) if at < nz - 2 else (0,)
        for d in range(1, nx):
            block = b * nx + lax.rem(x + d, nx)
            for i in range(2):
                w_arrived(block, i)
            if not whole:
                project(block, which=which)
        if whole:
            project(b * nx, first=at == 0, size=nx, which=which)

    for step in range(1, nz):
        pass_z(step, 0)
        if step == 2:
            pass_rows(1)
            for a in range(2):
                for d in range(chips):
                    row_arrived(a, lax.rem(chip + d, chips) * CORES + (CORES - 1 - core))
            if not whole:
                project(me, first=True)
            project_z(1)
        if step > 2:
            from_x(step - 2)
        pass_z(step, 1)
        if step == 1:
            pass_rows(0)
        else:
            if step == 2:
                from_x(0)
            if step == nz - 2:
                for d in range(1, nx):
                    swap_copy(d).start()
            project_z(step)
    for at in range(nz - 2, nz):
        from_x(at)

    own_c.wait()
    lanes = 128

    tap_lanes = pl.ds(pl.multiple_of(tp * cols, 128), cols)
    taps[0:3, 0:cols] = uptaps_ref[:, tap_lanes].astype(F32)
    taps[0:3, cols:both] = gatetaps_ref[:, tap_lanes].astype(F32)

    def taps_of(at):
        return [taps[k : k + 1, at] for k in range(3)]

    def conv(values, taps, row):
        return taps[2] * values + taps[1] * delayed(values, 1, row) + taps[0] * delayed(values, 2, row)

    def conv_back(grads, taps, row):
        return taps[2] * grads + taps[1] * advanced(grads, 1, row) + taps[0] * advanced(grads, 2, row)

    tloc[...] = jnp.zeros_like(tloc)

    def backward(j, carry):
        row = lax.broadcasted_iota(jnp.int32, (seq, lanes), 0)
        at_u = pl.ds(pl.multiple_of(j * lanes, lanes), lanes)
        at_g = pl.ds(pl.multiple_of(cols + j * lanes, lanes), lanes)
        tu, tg = taps_of(at_u), taps_of(at_g)
        vu = acc_s[:, at_u].astype(BF16).astype(F32)
        vg = acc_s[:, at_g].astype(BF16).astype(F32)
        cu, cg = conv(vu, tu, row), conv(vg, tg, row)
        sig = jax.nn.sigmoid(cg)
        upstream = cot[:, at_u].astype(F32)
        gu = upstream * (cg * sig)
        gg = upstream * cu * sig * (1.0 + cg * (1.0 - sig))
        gproj[:, at_u] = conv_back(gu, tu, row).astype(BF16)
        gproj[:, at_g] = conv_back(gg, tg, row).astype(BF16)
        for k, g, v in ((0, gu, vu), (3, gg, vg)):
            tloc[k : k + 1, at_u] = jnp.sum(g * delayed(v, 2, row), axis=0, keepdims=True)
            tloc[k + 1 : k + 2, at_u] = jnp.sum(g * delayed(v, 1, row), axis=0, keepdims=True)
            tloc[k + 2 : k + 3, at_u] = jnp.sum(g * v, axis=0, keepdims=True)
        return carry

    lax.fori_loop(0, cols // lanes, backward, 0)

    def weight_term(b, size=1):
        rows_of = size * depth
        left = rows_s[:, pl.ds(pl.multiple_of(b * depth, rows_of), rows_of)].T
        step = tile_of(both)

        def body(j, carry):
            tile = pl.ds(pl.multiple_of(j * step, step), step)
            term = jnp.dot(left, gproj[:, tile], preferred_element_type=F32).astype(BF16)
            for i in range(size):
                gbuf[b + i, :, tile] = term[i * depth : (i + 1) * depth]
            return carry

        lax.fori_loop(0, both // step, body, 0)

    fars = [far_order(at, nz) for at in range(nz)]
    order = [pick(z, [o[q] for o in fars]) for q in range(nz)]

    def hrows(i):
        return pl.ds(i * half, half)

    def x_grad(b, d, i):
        to = lax.rem(x + d, nx)
        return remote(
            gbuf.at[b * nx + to, hrows(i), :], xrecv.at[d - 1, b, hrows(i), :],
            x_send.at[d - 1, b, i], x_recv.at[d - 1, b, i], z * nx + to, tp,
        )

    def swap_grad(d):
        return remote(
            gbuf.at[pair * nx + lax.rem(x + d, nx), hrows(1), :], swrecv.at[d - 1],
            sw_send.at[d - 1], sw_recv.at[d - 1], pair * nx + x, tp,
        )

    def terms_of(b):
        if whole:
            weight_term(b * nx, size=nx)
        else:
            for d in range(1, nx):
                weight_term(b * nx + lax.rem(x + d, nx))

    def tap_x(d):
        return remote(
            tloc, trecv.at[d - 1], t_send.at[d - 1], t_recv.at[d - 1], z * nx + lax.rem(x + d, nx), tp
        )

    for d in range(1, nx):
        tap_x(d).start()

    for q in range(nz):
        b = order[q]
        if q == 0:
            terms_of(b)
        else:

            @pl.when(b != pair)
            def _():
                terms_of(b)

        for d in range(1, nx):
            x_grad(b, d, 0).start()

            if q < nz - 1:

                @pl.when(b != pair)
                def _():
                    x_grad(b, d, 1).start()

        if q == 0:
            terms_of(pair)
            for d in range(1, nx):
                swap_grad(d).start()
    for q in range(nz):
        if not whole:
            weight_term(order[q] * nx + x)

    def input_term(t):
        at = pl.ds(pl.multiple_of(t * part, part), part)
        step = tile_of(width)

        def body(j, carry):
            tile = pl.ds(pl.multiple_of(j * step, step), step)
            term = lax.dot_general(
                gproj[at, :], weights[tile, :], (((1,), (1,)), ((), ())), preferred_element_type=F32
            )
            pbuf[t, :, tile] = term.astype(BF16)
            return carry

        lax.fori_loop(0, width // step, body, 0)

    def part_copy(d):
        to = lax.rem(tp + d, nt)
        return remote(pbuf.at[to], precv.at[d - 1], p_send.at[d - 1], p_recv.at[d - 1], me, to)

    def all_input_terms():
        for d in range(1, nt):
            input_term(lax.rem(tp + d, nt))
            part_copy(d).start()
        input_term(tp)

    def forward(j, carry):
        row = lax.broadcasted_iota(jnp.int32, (seq, lanes), 0)
        at_u = pl.ds(pl.multiple_of(j * lanes, lanes), lanes)
        at_g = pl.ds(pl.multiple_of(cols + j * lanes, lanes), lanes)
        cu = conv(acc_l[:, at_u].astype(BF16).astype(F32), taps_of(at_u), row)
        cg = conv(acc_l[:, at_g].astype(BF16).astype(F32), taps_of(at_g), row)
        hidden_ref[:, at_u] = (cg * jax.nn.sigmoid(cg) * cu).astype(BF16)
        return carry

    def all_hidden():
        for at in range(nz - 2, nz):
            b = pick(z, [order[at] for order in nears])
            if whole:
                project(b * nx, size=nx, which=(1,))
            else:
                for d in range(1, nx):
                    project(b * nx + lax.rem(x + d, nx), which=(1,))
        lax.fori_loop(0, cols // lanes, forward, 0)

    total = tloc[...]
    for d in range(1, nx):
        tap_x(d).wait_recv()
        total = total + trecv[d - 1]
    tzrecv[nz - 1] = total

    def tap_z(d):
        return remote(
            tzrecv.at[nz - 1], tzrecv.at[d - 1], tz_send.at[d - 1], tz_recv.at[d - 1],
            lax.rem(z + d, nz) * nx + x, tp,
        )

    def tap_full(d):
        return remote(
            tapsum.at[tp], tapsum.at[tp], tt_send.at[d - 1], tt_recv.at[tp], me, lax.rem(tp + d, nt)
        )

    for d in range(1, nz):
        tap_z(d).start()

    def add_into(b, i, sources):
        value = gbuf[b, hrows(i), :].astype(F32)
        for source in sources:
            value = value + source[...].astype(F32)
        gbuf[b, hrows(i), :] = value.astype(BF16)

    def up_grad(b, i):
        return remote(
            gbuf.at[b * nx + x, hrows(i), :], uprecv.at[b, hrows(i), :],
            up_send.at[b, i], up_recv.at[b, i], me + nx, tp,
        )

    def dn_grad(b, i):
        return remote(
            gbuf.at[b * nx + x, hrows(i), :], dnrecv.at[b, hrows(i), :],
            dn_send.at[b, i], dn_recv.at[b, i], me - nx, tp,
        )

    for q in range(nz):
        b = order[q]
        mine = b * nx + x
        for i in range(2):
            if q < nz - 1:

                def from_x():
                    for d in range(1, nx):
                        x_grad(b, d, i).wait_recv()
                    add_into(mine, i, [xrecv.at[d - 1, b, hrows(i), :] for d in range(1, nx)])

                if i == 0:
                    from_x()
                else:
                    pl.when(b != pair)(from_x)

                @pl.when(b > z)
                def _():
                    @pl.when(z > 0)
                    def _():
                        up_grad(b, i).wait_recv()
                        add_into(mine, i, [uprecv.at[b, hrows(i), :]])

                    up_grad(b, i).start()

                @pl.when(b < z)
                def _():
                    @pl.when(z < nz - 1)
                    def _():
                        dn_grad(b, i).wait_recv()
                        add_into(mine, i, [dnrecv.at[b, hrows(i), :]])

                    dn_grad(b, i).start()

                continue
            if i == 0:
                for copy in own_s:
                    copy.wait()
            sides = ((newup_ref, 0, pl.ds(0, cols)), (newgate_ref, 1, pl.ds(cols, cols)))
            for d in range(1, nx):
                x_grad(b, d, i).wait_recv()
            for new, at, lane in sides:
                value = gbuf[mine, hrows(i), lane].astype(F32)
                for d in range(1, nx):
                    value = value + xrecv[d - 1, b, hrows(i), lane].astype(F32)
                new[hrows(i), :] = oldsum[at, hrows(i), :] + scale * value

            @pl.when(z > 0)
            def _():
                up_grad(b, i).wait_recv()
                for new, at, lane in sides:
                    new[hrows(i), :] += scale * uprecv[b, hrows(i), lane].astype(F32)

            @pl.when(z < nz - 1)
            def _():
                dn_grad(b, i).wait_recv()
                for new, at, lane in sides:
                    new[hrows(i), :] += scale * dnrecv[b, hrows(i), lane].astype(F32)

        if q == 0:
            for d in range(1, nx):
                swap_grad(d).wait_recv()
                add_into(z * nx + lax.rem(x + d, nx), 1, [swrecv.at[d - 1]])
                x_grad(z, d, 1).start()
            all_input_terms()
        if q == 1:
            all_hidden()
        if q == 0:
            total = tzrecv[nz - 1]
            for d in range(1, nz):
                tap_z(d).wait_recv()
                total = total + tzrecv[d - 1]
            tapsum[tp] = total
            for d in range(1, nt):
                tap_full(d).start()

    total = pbuf[tp].astype(F32)
    for d in range(1, nt):
        part_copy(d).wait_recv()
        total = total + precv[d - 1].astype(F32)
    ingrad_ref[...] = total.astype(BF16)

    for d in range(1, nt):
        from_tp = lax.rem(tp + d, nt)
        remote(
            tapsum.at[tp], tapsum.at[from_tp], tt_send.at[d - 1], tt_recv.at[from_tp], me, from_tp
        ).wait_recv()
        tap_full(d).wait_send()
        part_copy(d).wait_send()
    for t in range(nt):
        lane = pl.ds(t * cols, cols)
        newupt_ref[:, lane] = uptsum_ref[:, lane] + scale * tapsum[t, 0:3]
        newgatet_ref[:, lane] = gatetsum_ref[:, lane] + scale * tapsum[t, 3:6]
    for d in range(1, nx):
        tap_x(d).wait_send()
    for d in range(1, nz):
        tap_z(d).wait_send()
    for copy in first_rows + forwards:
        copy.wait_send()
    for d in range(1, nx):
        swap_copy(d).wait_send()
        swap_grad(d).wait_send()
    for b in range(nz):
        for i in range(2):

            def x_left():
                for copy in x_copies(b, i):
                    copy.wait_send()
                for d in range(1, nx):
                    x_grad(b, d, i).wait_send()

            if i == 0:
                x_left()
            else:
                pl.when(b != pair)(x_left)

            @pl.when(jnp.logical_and(z < nz - 1, b <= z))
            def _():
                up_copy(b, i).wait_send()

            @pl.when(jnp.logical_and(z > 0, b >= z))
            def _():
                dn_copy(b, i).wait_send()

            @pl.when(b > z)
            def _():
                up_grad(b, i).wait_send()

            @pl.when(b < z)
            def _():
                dn_grad(b, i).wait_send()


def shards(
    nf, nt,
    later_input, saved_input, cotangent, up_weight, gate_weight,
    up_taps, gate_taps, up_grad_sum, gate_grad_sum, up_taps_sum, gate_taps_sum,
):
    nx = 1 << ((nf.bit_length() - 1) // 2)
    nz = nf // nx
    depth, cols = up_weight.shape
    both = 2 * cols
    part, width = later_input.shape
    seq = part * nt
    scale = float(part * nf * nt) ** (-0.5)
    total_cols = up_taps.shape[1]
    dma = pltpu.SemaphoreType.DMA
    vmem = pl.BlockSpec(memory_space=pltpu.VMEM)
    hbm = pl.BlockSpec(memory_space=pl.ANY)
    return pl.pallas_call(
        functools.partial(kernel, nx, nz, nt, scale),
        out_shape=(
            jax.ShapeDtypeStruct((seq, cols), BF16),
            jax.ShapeDtypeStruct((part, width), BF16),
            jax.ShapeDtypeStruct((depth, cols), F32),
            jax.ShapeDtypeStruct((depth, cols), F32),
            jax.ShapeDtypeStruct((3, total_cols), F32),
            jax.ShapeDtypeStruct((3, total_cols), F32),
        ),
        in_specs=[hbm] * 7 + [vmem] * 4,
        out_specs=(vmem,) * 6,
        scratch_shapes=[
            pltpu.VMEM((width, both), BF16),
            pltpu.VMEM((seq, width), BF16),
            pltpu.VMEM((seq, width), BF16),
            pltpu.VMEM((seq, cols), BF16),
            pltpu.VMEM((seq, both), F32),
            pltpu.VMEM((seq, both), F32),
            pltpu.VMEM((seq, both), BF16),
            pltpu.VMEM((nf, depth, both), BF16),
            pltpu.VMEM((nx - 1, nz, depth, both), BF16),
            pltpu.VMEM((nz, depth, both), BF16),
            pltpu.VMEM((nz, depth, both), BF16),
            pltpu.VMEM((nx - 1, depth // 2, both), BF16),
            pltpu.VMEM((nt, part, width), BF16),
            pltpu.VMEM((nt - 1, part, width), BF16),
            pltpu.VMEM((2, depth, cols), F32),
            pltpu.VMEM((8, both), F32),
            pltpu.VMEM((8, cols), F32),
            pltpu.VMEM((nx - 1, 8, cols), F32),
            pltpu.VMEM((nz, 8, cols), F32),
            pltpu.VMEM((nt, 8, cols), F32),
            dma((7,)),
            dma((nf, 2)),
            dma((nz, 2)),
            dma((nz, 2)),
            dma((nx - 1, nz, 2)),
            dma((nx - 1,)),
            dma((2, nt)),
            dma((2, nt)),
            dma((2, nt)),
            dma((nx - 1, nz, 2)),
            dma((nx - 1, nz, 2)),
            dma((nx - 1,)),
            dma((nx - 1,)),
            dma((nz, 2)),
            dma((nz, 2)),
            dma((nz, 2)),
            dma((nz, 2)),
            dma((nt - 1,)),
            dma((nt - 1,)),
            dma((nx - 1,)),
            dma((nx - 1,)),
            dma((nz - 1,)),
            dma((nz - 1,)),
            dma((nt - 1,)),
            dma((nt,)),
        ],
        compiler_params=pltpu.CompilerParams(
            collective_id=0, has_side_effects=True, vmem_limit_bytes=67043328
        ),
        name="layer",
    )(
        later_input, saved_input, cotangent, up_weight, gate_weight, up_grad_sum, gate_grad_sum,
        up_taps, gate_taps, up_taps_sum, gate_taps_sum,
    )


def solution(mesh):
    return jax.shard_map(
        functools.partial(shards, mesh.shape["fs"], mesh.shape["tp"]),
        mesh=mesh,
        in_specs=(
            P(("fs", "tp"), None),
            P(("fs", "tp"), None),
            P("fs", "tp"),
            P("fs", "tp"),
            P("fs", "tp"),
            P(),
            P(),
            P("fs", "tp"),
            P("fs", "tp"),
            P(),
            P(),
        ),
        out_specs=(P("fs", "tp"), P(("fs", "tp"), None), P("fs", "tp"), P("fs", "tp"), P(), P()),
        check_vma=False,
    )
```
